512 devices in a mesh: kv: 64 (over z, y), tp: 8 (over x, core).
Axes of the slice: x: 4, y: 8, z: 8, core: 2. Of those that a mesh axis runs over, the one named last changes fastest.
Arguments:
- tokens: bfloat16 [16, 4096], P(None, 'kv'), may hold values from -32 to 32
- attn_gain: float32 [4096], P('kv'), may hold values from 0.1 to 1.9
- w_query: bfloat16 [4096, 4096], P('kv', 'tp'), may hold values from -0.09375 to 0.09375
- w_key: bfloat16 [4096, 4096], P('kv', 'tp'), may hold values from -0.09375 to 0.09375
- w_value: bfloat16 [4096, 4096], P('kv', 'tp'), may hold values from -0.09375 to 0.09375
- key_cache: bfloat16 [16, 8192, 32, 128], P(None, 'kv', 'tp'), may hold values from -128 to 128
- value_cache: bfloat16 [16, 8192, 32, 128], P(None, 'kv', 'tp'), may hold values from -6 to 6
- lengths: int32 [16], replicated, may hold values from 1 to 8192, as said below
- mix_weight: float32 [32], P('tp'), may hold values from 0.3 to 0.8
- head_gain: float32 [128], replicated, may hold values from 0.1 to 1.9
- w_out: bfloat16 [4096, 4096], P('tp', 'kv'), may hold values from -0.09375 to 0.09375
- mixer_gain: float32 [4096], P('kv'), may hold values from 0.1 to 1.9
- w_gate: bfloat16 [4096, 11264], P('kv', 'tp'), may hold values from -0.09375 to 0.09375
- w_up: bfloat16 [4096, 11264], P('kv', 'tp'), may hold values from -0.09375 to 0.09375
- w_down: bfloat16 [11264, 4096], P('tp', 'kv'), may hold values from -0.0546875 to 0.0546875
Outputs:
- layer_out: bfloat16 [16, 4096], P(None, 'kv')
The draws below stay inside these ranges and needn't reach their ends.
Inputs may be any that keep to these rules, and one draw needn't show every extreme that they name: `lengths`: one sequence has exactly 8192 live positions; four or more sequences, a quarter of them or more, have 4 or fewer.
All inputs are finite; a program needn't handle non-finite values.
Results may differ from the reference program's by a relative error of at most 0.017.
Values may be sent and summed in bfloat16 or wider, within the bound.
No kernel may reach another device: no remote copies, remote signals or barrier semaphores. Data moves between devices by JAX's collectives and lax.ppermute only.
A program may use at most 64 MiB of HBM per device.

```python
import jax
import jax.numpy as jnp
from jax import lax

D = 4096
H = 32
DH = 64
DV = 128
FF = 11264
BATCH = 16
LENGTH = 8192
N_TP = 8


def draw_tokens(key, part):
    first_key, second_key = jax.random.split(key, 2)
    columns = jnp.arange(D, dtype=jnp.float32) / D
    roughness = jnp.exp(jax.random.uniform(second_key, (D,), jnp.float32, -0.7, 0.7))
    column_scale = 3.0 ** columns * roughness
    base_values = jnp.clip(jax.random.normal(first_key, (BATCH, D), jnp.float32), -4.0, 4.0)
    values = base_values * column_scale[None, :]
    return values.astype(jnp.bfloat16)


def draw_key_cache(key, part):
    first_key = jax.random.fold_in(key, 0)
    values = jnp.clip(jax.random.normal(first_key, (BATCH, LENGTH, H, 2 * DH), jnp.float32) * 1.75, -10.5, 10.5)
    return values.astype(jnp.bfloat16)


def draw_lengths(key, part):
    order_key, short_key, middle_key = jax.random.split(jax.random.fold_in(key, 7), 3)
    short_count = max(4, BATCH // 4)
    rank = jnp.arange(BATCH, dtype=jnp.int32)
    short_values = jax.random.randint(short_key, (BATCH,), 1, 5, dtype=jnp.int32)
    short_values = jnp.where(rank == 1, jnp.int32(1), short_values)
    middle_values = jax.random.randint(middle_key, (BATCH,), LENGTH // 8, LENGTH // 2 + 1, dtype=jnp.int32)
    full_values = jnp.full((BATCH,), LENGTH, dtype=jnp.int32)
    ranked = jnp.where(rank == 0, full_values, jnp.where(rank <= short_count, short_values, middle_values))
    order = jax.random.permutation(order_key, BATCH).astype(jnp.int32)
    return ranked[order].astype(jnp.int32)


def shard_levels(own_key, shape, shards, least, largest):
    gain = 1.0
    for axis_at, shards_of in shards:
        draws = jax.random.uniform(jax.random.fold_in(jax.random.fold_in(own_key, 6), axis_at), (shards_of,), jnp.float32, least / len(shards), largest / len(shards))
        gain = gain * jnp.repeat(jnp.exp(draws), shape[axis_at] // shards_of).reshape((-1,) + (1,) * (len(shape) - 1 - axis_at))
    return gain


def bell_draw(stream_key, shape, scale, reach, pieces=(), kind=jnp.bfloat16):
    entries = scale * jax.random.normal(stream_key, shape, jnp.float32)
    if pieces:
        entries = entries * shard_levels(stream_key, shape, pieces, -0.22, 0.18)
    return jnp.clip(entries, -reach, reach).astype(kind)


def setup_inputs(seed: int = 0) -> dict:
    arg_keys = jax.random.split(jax.random.key(seed), 16)
    tokens = draw_tokens(jax.random.fold_in(arg_keys[15], 71), 0)
    attn_gain = jnp.clip(1.0 + 0.18 * jax.random.normal(arg_keys[1], (D,), jnp.float32), 0.1, 1.9)
    w_query = bell_draw(arg_keys[2], (D, H * 2 * DH), D ** -0.5, 0.09375, ((0, 64), (1, 8)))
    w_key = bell_draw(arg_keys[3], (D, H * 2 * DH), D ** -0.5, 0.09375, ((0, 64), (1, 8)))
    w_value = bell_draw(arg_keys[4], (D, H * DV), D ** -0.5, 0.09375, ((0, 64), (1, 8)))
    key_cache = draw_key_cache(jax.random.fold_in(arg_keys[15], 71), 0)
    value_cache = bell_draw(arg_keys[6], (BATCH, LENGTH, H, DV), 1.0, 6.0, ((1, 64), (2, 8)))
    lengths = draw_lengths(jax.random.fold_in(arg_keys[15], 71), 0)
    mix_weight = jnp.clip(0.3 + 0.5 * jax.random.uniform(arg_keys[8], (H,), jnp.float32) ** shard_levels(arg_keys[8], (H,), ((0, 8),), -0.2, 0.2), 0.3, 0.8)
    head_gain = jnp.clip(1.0 + 0.18 * jax.random.normal(arg_keys[9], (DV,), jnp.float32), 0.1, 1.9)
    w_out = bell_draw(arg_keys[10], (H * DV, D), (H * DV) ** -0.5, 0.09375, ((0, 8), (1, 64)))
    mixer_gain = jnp.clip(1.0 + 0.18 * jax.random.normal(arg_keys[11], (D,), jnp.float32), 0.1, 1.9)
    w_gate = bell_draw(arg_keys[12], (D, FF), D ** -0.5, 0.09375, ((0, 64), (1, 8)))
    w_up = bell_draw(arg_keys[13], (D, FF), D ** -0.5, 0.09375, ((0, 64), (1, 8)))
    w_down = bell_draw(arg_keys[14], (FF, D), FF ** -0.5, 0.0546875, ((0, 8), (1, 64)))
    return dict(tokens=tokens, attn_gain=attn_gain, w_query=w_query, w_key=w_key, w_value=w_value, key_cache=key_cache, value_cache=value_cache, lengths=lengths, mix_weight=mix_weight, head_gain=head_gain, w_out=w_out, mixer_gain=mixer_gain, w_gate=w_gate, w_up=w_up, w_down=w_down)


EPS = 1e-06

def rounded(values):
    return lax.optimization_barrier(values.astype(jnp.bfloat16)).astype(jnp.float32)

def one_sequence(queries, key_new, value_new, key_rows, value_rows, seq_length, mix_weight, head_gain):
    logit_scale = DH ** (-0.5)
    query_float = queries.astype(jnp.float32).reshape(H, 2, DH)
    keys_float = key_rows.astype(jnp.float32).reshape(LENGTH, H, 2, DH)
    score_matrix = jnp.einsum('crx,ecrx->cre', query_float, keys_float) * logit_scale
    own_score = lax.optimization_barrier(jnp.sum(query_float * key_new.astype(jnp.float32).reshape(H, 2, DH), axis=2)) * logit_scale
    visible = (jnp.arange(LENGTH, dtype=jnp.int32) < seq_length)[None, None, :]
    peak_score = jnp.maximum(lax.optimization_barrier(jnp.max(jnp.where(visible, score_matrix, -jnp.inf), axis=2)), own_score)
    weights = jnp.where(visible, jnp.exp(score_matrix - peak_score[:, :, None]), 0.0)
    own_weight = jnp.exp(own_score - peak_score)
    totals = lax.optimization_barrier(jnp.sum(weights, axis=2)) + own_weight
    accumulated = jnp.einsum('hmp,phv->hmv', rounded(weights), value_rows.astype(jnp.float32))
    accumulated = accumulated + rounded(own_weight)[:, :, None] * value_new.astype(jnp.float32).reshape(H, 1, DV)
    mixture = accumulated[:, 0] / totals[:, 0, None] - mix_weight[:, None] * accumulated[:, 1] / totals[:, 1, None]
    head_scale = lax.rsqrt(lax.optimization_barrier(jnp.mean(mixture * mixture, axis=1, keepdims=True)) + EPS)
    return (mixture * head_scale * head_gain.astype(jnp.float32)).astype(jnp.bfloat16).reshape(H * DV)

def blocked_sum(left_side, right_side, group_count):
    row_count = left_side.shape[0]
    inner_size = left_side.shape[1] // group_count
    partial_terms = jnp.einsum('bgi,gid->gbd', left_side.astype(jnp.float32).reshape(row_count, group_count, inner_size), right_side.astype(jnp.float32).reshape(group_count, inner_size, right_side.shape[1]))
    return lax.optimization_barrier(jnp.sum(rounded(partial_terms), axis=0))

def reference(tokens, attn_gain, w_query, w_key, w_value, key_cache, value_cache, lengths, mix_weight, head_gain, w_out, mixer_gain, w_gate, w_up, w_down):
    tokens_float = tokens.astype(jnp.float32)
    inverse = lax.rsqrt(lax.optimization_barrier(jnp.mean(tokens_float * tokens_float, axis=1, keepdims=True)) + EPS)
    scaled = (tokens_float * attn_gain.astype(jnp.float32)).astype(jnp.bfloat16)
    queries = (inverse * jnp.dot(scaled, w_query, preferred_element_type=jnp.float32)).astype(jnp.bfloat16)
    key_new = (inverse * jnp.dot(scaled, w_key, preferred_element_type=jnp.float32)).astype(jnp.bfloat16)
    value_new = (inverse * jnp.dot(scaled, w_value, preferred_element_type=jnp.float32)).astype(jnp.bfloat16)

    def per_sequence(inputs):
        return one_sequence(inputs[0], inputs[1], inputs[2], inputs[3], inputs[4], inputs[5], mix_weight.astype(jnp.float32), head_gain)
    attended = lax.map(per_sequence, (queries, key_new, value_new, key_cache, value_cache, lengths.astype(jnp.int32)))
    residual = (tokens_float + blocked_sum(attended, w_out, N_TP)).astype(jnp.bfloat16)
    residual_f = residual.astype(jnp.float32)
    reciprocal_mixture = lax.rsqrt(lax.optimization_barrier(jnp.mean(residual_f * residual_f, axis=1, keepdims=True)) + EPS)
    scaled_mix = (residual_f * mixer_gain.astype(jnp.float32)).astype(jnp.bfloat16)
    gate = reciprocal_mixture * jnp.dot(scaled_mix, w_gate, preferred_element_type=jnp.float32)
    up_proj = reciprocal_mixture * jnp.dot(scaled_mix, w_up, preferred_element_type=jnp.float32)
    hidden = (jax.nn.silu(gate) * up_proj).astype(jnp.bfloat16)
    return (residual_f + blocked_sum(hidden, w_down, N_TP)).astype(jnp.bfloat16)
```

```python
import jax
import jax.numpy as jnp
from jax import lax
from jax.experimental import pallas as pl
from jax.experimental.pallas import tpu as pltpu
from jax.sharding import Mesh
from jax.sharding import PartitionSpec as P

KV = ("z", "y")
EPS = 1e-06
FLOOR_SCORE = -1e30
BF = jnp.bfloat16
F32 = jnp.float32
VMEM = pl.BlockSpec(memory_space=pltpu.VMEM)
SMEM = pl.BlockSpec(memory_space=pltpu.SMEM)
INTERPRET = False


def run(kernel, outs, args, scalars=0, scratch=()):
    single = not isinstance(outs, (list, tuple))
    return pl.pallas_call(
        kernel,
        out_shape=outs,
        in_specs=[SMEM] * scalars + [VMEM] * (len(args) - scalars),
        out_specs=VMEM if single else [VMEM] * len(outs),
        scratch_shapes=scratch,
        interpret=INTERPRET,
    )(*args)


def shape(*dims, kind=BF):
    return jax.ShapeDtypeStruct(dims, kind)


def exchange(array, axis):
    return lax.all_to_all(array, axis, 0, 0, tiled=True)


def dot(left, right):
    return jnp.dot(left, right, preferred_element_type=F32)


def dot_t(left, right):
    return lax.dot_general(left, right, (((1,), (1,)), ((), ())), preferred_element_type=F32)


def rounded(array):
    return array.astype(BF).astype(F32)


def summed(ref):
    total = ref[0].astype(F32)
    for i in range(1, ref.shape[0]):
        total = total + ref[i].astype(F32)
    return total


def iota(shape_, dim):
    return lax.broadcasted_iota(jnp.int32, shape_, dim)


def project(tokens, gain, w_query, w_key, w_value, out):
    x = tokens[...].astype(F32)
    scaled = (x * gain[...]).astype(BF)
    query = dot(scaled, w_query[...]).astype(BF)
    key = dot(scaled, w_key[...])
    value = dot(scaled, w_value[...])
    squares = jnp.broadcast_to(jnp.sum(x * x, axis=1, keepdims=True), (16, 128)).astype(BF)
    for y in range(8):
        rows = slice(8 * (y // 4), 8 * (y // 4) + 8)
        lanes = slice(128 * (y % 4), 128 * (y % 4) + 128)
        out[y, :, 0:512] = query
        out[y, :, 512:640] = jnp.concatenate([key[rows, lanes], value[rows, lanes]], axis=0).astype(BF)
        out[y, :, 640:768] = squares


def relay(got, out):
    total = summed(got).astype(BF)
    for i in range(8):
        out[i] = total


def attend(place, lengths, got, keys, values, out, rows_q, rows_k, rows_v, acc, stat):
    z, half, head = place[0], place[1] // 4, place[1] % 4
    start = (place[0] * 8 + place[1]) * 128
    total = summed(got)
    inverse = lax.rsqrt(total[:, 640:768] / 4096 + EPS)
    first = iota((16, 128), 1) < 64
    for h in range(4):
        query = rounded(inverse * total[:, 128 * h : 128 * h + 128])
        rows_q[pl.ds(2 * h, 16, stride=8), :] = jnp.where(first, query, 0.0)
        rows_q[pl.ds(2 * h + 1, 16, stride=8), :] = jnp.where(first, 0.0, query)
    inverse_half = jnp.where(half == 0, inverse[0:8], inverse[8:16])
    key_new = rounded(inverse_half * total[0:8, 512:640])
    value_new = rounded(inverse_half * total[8:16, 512:640])
    for part in range(2):
        for h in range(4):
            mine = jnp.logical_and(z == 0, jnp.logical_and(half == part, head == h))
            for m in range(2):
                at = pl.ds(64 * part + 2 * h + m, 8, stride=8)
                rows_k[at, :] = jnp.where(mine, key_new, 0.0)
                rows_v[at, :] = jnp.where(mine, value_new, 0.0)
    row = iota((8, 512), 0)
    column = iota((8, 512), 1)
    same_head = (column & 3) == (row >> 1)
    position = column >> 2
    owner_row = jnp.logical_and(z == 0, (iota((8, 1), 0) >> 1) == head)
    lane = iota((8, 128), 1)
    for b in range(16):
        at = slice(8 * b, 8 * b + 8)
        query = rows_q[at, :]
        scores = dot_t(query.astype(BF), keys[b]) * 0.125
        visible = jnp.logical_and(same_head, position < lengths[b] - start)
        scores = jnp.where(visible, scores, FLOOR_SCORE)
        owner = jnp.logical_and(owner_row, half == b // 8)
        own = jnp.sum(query * rows_k[at, :], axis=1, keepdims=True) * 0.125
        own = jnp.where(owner, own, FLOOR_SCORE)
        peak = jnp.maximum(jnp.max(scores, axis=1, keepdims=True), own)
        peak_hi = rounded(peak)
        peak_lo = rounded(peak - peak_hi)
        base = peak_hi + peak_lo
        weights = jnp.where(visible, jnp.exp(scores - base), 0.0)
        own_weight = jnp.where(owner, jnp.exp(own - base), 0.0)
        totals = jnp.sum(weights, axis=1, keepdims=True) + own_weight
        acc[at, :] = dot(weights.astype(BF), values[b]) + rounded(own_weight) * rows_v[at, :]
        totals_hi = rounded(totals)
        stat[at, :] = jnp.where(
            lane == 0,
            peak_hi,
            jnp.where(lane == 1, peak_lo, jnp.where(lane == 2, totals_hi, totals - totals_hi)),
        )
    body = acc[...].T.astype(BF)
    tail = stat[...].T[0:8].astype(BF)
    for i in range(8):
        out[i, 0:128, :] = body
        out[i, 128:136, :] = tail


def merged(got):
    tails = [got[i, 128:136, :].astype(F32) for i in range(8)]
    peaks = [t[0:1] + t[1:2] for t in tails]
    peak = peaks[0]
    for p in peaks[1:]:
        peak = jnp.maximum(peak, p)
    totals = jnp.zeros_like(peak)
    values = jnp.zeros((128, 128), F32)
    for i in range(8):
        scale = jnp.exp(peaks[i] - peak)
        totals = totals + scale * (tails[i][2:3] + tails[i][3:4])
        values = values + scale * got[i, 0:128, :].astype(F32)
    return peak, totals, values


def merge(got, out):
    peak, totals, values = merged(got)
    peak_hi, totals_hi = rounded(peak), rounded(totals)
    row = iota((8, 128), 0)
    tail = jnp.where(
        row == 0,
        peak_hi,
        jnp.where(row == 1, peak - peak_hi, jnp.where(row == 2, totals_hi, totals - totals_hi)),
    ).astype(BF)
    body = values.astype(BF)
    for i in range(8):
        out[i, 0:128, :] = body
        out[i, 128:136, :] = tail


def mix(weight, got, head_gain, w_out, out, rows):
    _, totals, values = merged(got)
    ratio = values / totals
    head = (iota((1, 128), 1) >> 1) & 3
    share = jnp.where(
        head == 0, weight[0], jnp.where(head == 1, weight[1], jnp.where(head == 2, weight[2], weight[3]))
    )
    mixture = ratio - share * pltpu.roll(ratio, 127, 1)
    scale = lax.rsqrt(jnp.mean(mixture * mixture, axis=0, keepdims=True) + EPS)
    rows[...] = (mixture * scale).T * head_gain[...]
    attended = jnp.concatenate(
        [rows[pl.ds(2 * h, 16, stride=8), :] for h in range(4)], axis=1
    ).astype(BF)
    term = dot_t(attended, w_out[...]).astype(BF)
    for i in range(8):
        out[i] = term


def widen(got, tokens, gain, w_gate, w_up, out, residual_out, rows):
    residual = (tokens[...].astype(F32) + summed(got)).astype(BF)
    residual_out[...] = residual
    x = residual.astype(F32)
    scaled = (x * gain[...]).astype(BF)
    gate = dot(scaled, w_gate[...])
    up = dot(scaled, w_up[...])
    squares = jnp.broadcast_to(jnp.sum(x * x, axis=1, keepdims=True), (16, 128))
    zeros = jnp.zeros((16, 128), F32)
    for tile in range(12):
        group, j = tile // 3, tile % 3
        lanes = slice(128 * tile, 128 * tile + 128)
        rows[pl.ds(8 * group + j, 16, stride=32), :] = gate[:, lanes] if tile < 11 else zeros
        rows[pl.ds(8 * group + 3 + j, 16, stride=32), :] = up[:, lanes] if tile < 11 else zeros
    for group in range(4):
        rows[pl.ds(8 * group + 6, 16, stride=32), :] = squares
        rows[pl.ds(8 * group + 7, 16, stride=32), :] = squares
    out[...] = rows[...].astype(BF)


def activate(got, out):
    total = summed(got)
    inverse = lax.rsqrt(total[6:7] / 4096 + EPS)
    gate = inverse * total[0:3]
    up = inverse * total[3:6]
    hidden = gate / (1.0 + jnp.exp(-gate)) * up
    hidden = jnp.concatenate([hidden, jnp.zeros((5, 128), F32)], axis=0).astype(BF)
    for i in range(64):
        out[i] = hidden


def narrow(got, w_down, out, rows):
    rows[...] = got[...].astype(F32)
    hidden = jnp.concatenate(
        [rows[pl.ds(8 * (t // 3) + t % 3, 16, stride=32), :] for t in range(11)], axis=1
    ).astype(BF)
    term = dot_t(hidden, w_down[...]).astype(BF)
    for i in range(8):
        out[i] = term


def local(
    tokens,
    attn_gain,
    w_query,
    w_key,
    w_value,
    key_cache,
    value_cache,
    lengths,
    mix_weight,
    head_gain,
    w_out,
    mixer_gain,
    w_gate,
    w_up,
    w_down,
):
    place = jnp.stack([lax.axis_index("z"), lax.axis_index("y")]).astype(jnp.int32)
    tile = pltpu.VMEM((128, 128), F32)
    wide = pltpu.VMEM((512, 128), F32)
    sent = run(project, shape(8, 16, 768), (tokens, attn_gain[None], w_query, w_key, w_value))
    sent = run(relay, shape(8, 16, 768), (exchange(sent, "y"),))
    sent = run(
        attend,
        shape(8, 136, 128),
        (
            place,
            lengths,
            exchange(sent, "z"),
            key_cache.reshape(16, 512, 128),
            value_cache.reshape(16, 512, 128),
        ),
        scalars=2,
        scratch=[tile] * 5,
    )
    sent = run(merge, shape(8, 136, 128), (exchange(sent, "y"),))
    sent = run(
        mix,
        shape(8, 16, 64),
        (mix_weight, exchange(sent, "z"), head_gain[None], w_out.T),
        scalars=1,
        scratch=[tile],
    )
    sent, residual = run(
        widen,
        (shape(512, 128), shape(16, 64)),
        (exchange(sent, "tp"), tokens, mixer_gain[None], w_gate, w_up),
        scratch=[wide],
    )
    sent = run(activate, shape(64, 8, 128), (exchange(sent.reshape(64, 8, 128), KV),))
    sent = run(
        narrow, shape(8, 16, 64), (exchange(sent, KV).reshape(512, 128), w_down.T), scratch=[wide]
    )
    terms = exchange(sent, "tp")
    return (residual.astype(F32) + jnp.sum(terms.astype(F32), axis=0)).astype(BF)


def solution(mesh):
    finer = Mesh(mesh.devices.reshape(8, 8, mesh.shape["tp"]), ("z", "y", "tp"))
    return jax.shard_map(
        local,
        mesh=finer,
        in_specs=(
            P(None, KV),
            P(KV),
            P(KV, "tp"),
            P(KV, "tp"),
            P(KV, "tp"),
            P(None, KV, "tp", None),
            P(None, KV, "tp", None),
            P(),
            P("tp"),
            P(),
            P("tp", KV),
            P(KV),
            P(KV, "tp"),
            P(KV, "tp"),
            P("tp", KV),
        ),
        out_specs=P(None, KV),
        check_vma=False,
    )
```

```python
import jax
import jax.numpy as jnp
from jax import lax
from jax.experimental import pallas as pl
from jax.experimental.pallas import tpu as pltpu
from jax.sharding import Mesh
from jax.sharding import PartitionSpec as P

KV = ("z", "y")
EPS = 1e-06
FLOOR_SCORE = -1e30
BF = jnp.bfloat16
F32 = jnp.float32
VMEM = pl.BlockSpec(memory_space=pltpu.VMEM)
HBM = pl.BlockSpec(memory_space=pltpu.HBM)
INTERPRET = False


def run(kernel, outs, args, specs=None, scratch=(), grant=4):
    single = not isinstance(outs, (list, tuple))
    specs = specs or [VMEM] * len(args)
    if not INTERPRET:
        args = [
            pltpu.with_memory_space_constraint(a, s.memory_space) for a, s in zip(args, specs)
        ]
    return pl.pallas_call(
        kernel,
        out_shape=outs,
        in_specs=specs,
        out_specs=VMEM if single else [VMEM] * len(outs),
        scratch_shapes=scratch,
        compiler_params=pltpu.CompilerParams(vmem_limit_bytes=grant << 20),
        interpret=INTERPRET,
    )(*args)


def shape(*dims, kind=BF):
    return jax.ShapeDtypeStruct(dims, kind) if INTERPRET else pltpu.VMEM(dims, kind)


def exchange(array, axis):
    return lax.all_to_all(array, axis, 0, 0, tiled=True)


def dot(left, right):
    return jnp.dot(left, right, preferred_element_type=F32)


def dot_t(left, right):
    return lax.dot_general(left, right, (((1,), (1,)), ((), ())), preferred_element_type=F32)


def rounded(array):
    return array.astype(BF).astype(F32)


def summed(ref):
    total = ref[0].astype(F32)
    for i in range(1, ref.shape[0]):
        total = total + ref[i].astype(F32)
    return total


def folded(term):
    return jnp.concatenate([term[0:8], term[8:16]], axis=1).astype(BF)


def unfolded(term):
    return jnp.concatenate([term[:, 0:64], term[:, 64:128]], axis=0)


def iota(shape_, dim):
    return lax.broadcasted_iota(jnp.int32, shape_, dim)


def project(
    tokens, gain, w_query, w_key, w_value, lengths, weight, keys, values,
    out, keys_out, values_out, limit, owner, share,
    tokens_in, gain_in, query_in, key_in, value_in, lengths_in, weight_in, sems,
):
    pairs = (
        (tokens, tokens_in),
        (gain, gain_in),
        (w_query, query_in),
        (w_key, key_in),
        (w_value, value_in),
        (lengths, lengths_in),
        (weight, weight_in),
        (keys, keys_out),
        (values, values_out),
    )
    copies = [pltpu.make_async_copy(a, b, sems.at[i]) for i, (a, b) in enumerate(pairs)]
    for copy in copies:
        copy.start()
    for copy in copies[:5]:
        copy.wait()
    x = tokens_in[...].astype(F32)
    scaled = (x * gain_in[...]).astype(BF)
    query = dot(scaled, query_in[...]).astype(BF)
    key = dot(scaled, key_in[...])
    value = dot(scaled, value_in[...])
    squares = jnp.broadcast_to(jnp.sum(x * x, axis=1, keepdims=True), (16, 128)).astype(BF)
    for y in range(8):
        rows = slice(8 * (y // 4), 8 * (y // 4) + 8)
        lanes = slice(128 * (y % 4), 128 * (y % 4) + 128)
        out[y, :, 0:512] = query
        out[y, :, 512:640] = jnp.concatenate([key[rows, lanes], value[rows, lanes]], axis=0).astype(BF)
        out[y, :, 640:768] = squares
    for copy in copies[5:7]:
        copy.wait()
    z, y = lax.axis_index("z"), lax.axis_index("y")
    half, head = y // 4, y % 4
    start = (z * 8 + y) * 128
    row_head = iota((8, 128), 0) >> 1
    same_head = (iota((8, 128), 1) & 3) == row_head
    for b in range(16):
        at = slice(8 * b, 8 * b + 8)
        limit[at, :] = jnp.where(same_head, lengths_in[b] - start, 0)
        mine = jnp.logical_and(z == 0, half == b // 8)
        owner[at, :] = jnp.where(jnp.logical_and(mine, row_head == head), 1, 0)
    lane_head = (iota((8, 128), 1) >> 1) & 3
    low = jnp.where(lane_head == 0, weight_in[0], weight_in[1])
    high = jnp.where(lane_head == 2, weight_in[2], weight_in[3])
    share[...] = jnp.where(lane_head < 2, low, high)
    for copy in copies[7:]:
        copy.wait()


def relay(got, out):
    total = summed(got).astype(BF)
    for i in range(8):
        out[i] = total


def attend(got, keys, values, limit, owner, out, rows_q, rows_k, rows_v, scores, acc):
    total = summed(got)
    inverse = lax.rsqrt(total[:, 640:768] / 4096 + EPS)
    first = iota((16, 128), 1) < 64
    for h in range(4):
        query = rounded(inverse * total[:, 128 * h : 128 * h + 128])
        rows_q[pl.ds(2 * h, 16, stride=8), :] = jnp.where(first, query, 0.0)
        rows_q[pl.ds(2 * h + 1, 16, stride=8), :] = jnp.where(first, 0.0, query)
    for b in range(16):
        at = slice(8 * b, 8 * b + 8)
        scores[at, :] = dot_t(rows_q[at, :].astype(BF), keys[b])
    for part in range(2):
        scale = inverse[8 * part : 8 * part + 8]
        key_new = rounded(scale * total[0:8, 512:640])
        value_new = rounded(scale * total[8:16, 512:640])
        for i in range(8):
            at = pl.ds(64 * part + i, 8, stride=8)
            rows_k[at, :] = key_new
            rows_v[at, :] = value_new
    owned = owner[...] > 0
    own = jnp.sum(rows_q[...] * rows_k[...], axis=1, keepdims=True) * 0.125
    own = jnp.where(owned, own, FLOOR_SCORE)
    lane = iota((128, 128), 1)
    tiles, seen = [], []
    peak = own
    for t in range(4):
        visible = (lane + 128 * t) >> 2 < limit[...]
        tile = jnp.where(visible, scores[:, 128 * t : 128 * t + 128] * 0.125, FLOOR_SCORE)
        tiles.append(tile)
        seen.append(visible)
        peak = jnp.maximum(peak, tile)
    peak = jnp.max(peak, axis=1, keepdims=True)
    peak_hi = rounded(peak)
    peak_lo = rounded(peak - peak_hi)
    base = peak_hi + peak_lo
    weights = [jnp.where(v, jnp.exp(t - base), 0.0) for t, v in zip(tiles, seen)]
    own_weight = jnp.where(owned, jnp.exp(own - base), 0.0)
    totals = jnp.sum(weights[0] + weights[1] + weights[2] + weights[3], axis=1, keepdims=True)
    totals = totals + own_weight
    weights = jnp.concatenate(weights, axis=1).astype(BF)
    for b in range(16):
        at = slice(8 * b, 8 * b + 8)
        acc[at, :] = dot(weights[at, :], values[b])
    body = (acc[...] + rounded(own_weight) * rows_v[...]).T.astype(BF)
    totals_hi = rounded(totals)
    stat = jnp.where(
        lane == 0,
        peak_hi,
        jnp.where(lane == 1, peak_lo, jnp.where(lane == 2, totals_hi, totals - totals_hi)),
    )
    tail = stat.T[0:8].astype(BF)
    for i in range(8):
        out[i, 0:128, :] = body
        out[i, 128:136, :] = tail


def merged(got):
    tails = [got[i, 128:136, :].astype(F32) for i in range(8)]
    peaks = [t[0:1] + t[1:2] for t in tails]
    peak = peaks[0]
    for p in peaks[1:]:
        peak = jnp.maximum(peak, p)
    totals = jnp.zeros_like(peak)
    values = jnp.zeros((128, 128), F32)
    for i in range(8):
        scale = jnp.exp(peaks[i] - peak)
        totals = totals + scale * (tails[i][2:3] + tails[i][3:4])
        values = values + scale * got[i, 0:128, :].astype(F32)
    return peak, totals, values


def merge(got, out):
    peak, totals, values = merged(got)
    peak_hi, totals_hi = rounded(peak), rounded(totals)
    row = iota((8, 128), 0)
    tail = jnp.where(
        row == 0,
        peak_hi,
        jnp.where(row == 1, peak - peak_hi, jnp.where(row == 2, totals_hi, totals - totals_hi)),
    ).astype(BF)
    body = values.astype(BF)
    for i in range(8):
        out[i, 0:128, :] = body
        out[i, 128:136, :] = tail


def mix(got, share, head_gain, w_out, out, rows):
    _, totals, values = merged(got)
    ratio = values / totals
    mixture = ratio - share[0:1] * pltpu.roll(ratio, 127, 1)
    scale = lax.rsqrt(jnp.mean(mixture * mixture, axis=0, keepdims=True) + EPS)
    rows[...] = (mixture * scale).T * head_gain[...]
    attended = jnp.concatenate(
        [rows[pl.ds(2 * h, 16, stride=8), :] for h in range(4)], axis=1
    ).astype(BF)
    term = folded(dot_t(attended, w_out[...]))
    for i in range(8):
        out[i] = term


def widen(got, tokens, gain, w_gate, w_up, out, residual_out, rows):
    residual = (tokens[...].astype(F32) + unfolded(summed(got))).astype(BF)
    residual_out[...] = residual
    x = residual.astype(F32)
    scaled = (x * gain[...]).astype(BF)
    gate = dot(scaled, w_gate[...])
    up = dot(scaled, w_up[...])
    squares = jnp.broadcast_to(jnp.sum(x * x, axis=1, keepdims=True), (16, 128))
    zeros = jnp.zeros((16, 128), F32)
    for tile in range(12):
        group, j = tile // 3, tile % 3
        lanes = slice(128 * tile, 128 * tile + 128)
        rows[pl.ds(8 * group + j, 16, stride=32), :] = gate[:, lanes] if tile < 11 else zeros
        rows[pl.ds(8 * group + 3 + j, 16, stride=32), :] = up[:, lanes] if tile < 11 else zeros
    for group in range(4):
        rows[pl.ds(8 * group + 6, 16, stride=32), :] = squares
        rows[pl.ds(8 * group + 7, 16, stride=32), :] = squares
    out[...] = rows[...].astype(BF)


def activate(got, out):
    total = summed(got)
    inverse = lax.rsqrt(total[6:7] / 4096 + EPS)
    gate = inverse * total[0:3]
    up = inverse * total[3:6]
    hidden = gate / (1.0 + jnp.exp(-gate)) * up
    hidden = jnp.concatenate([hidden, jnp.zeros((5, 128), F32)], axis=0).astype(BF)
    for i in range(64):
        out[i] = hidden


def narrow(got, w_down, out, rows):
    rows[...] = got[...].astype(F32)
    hidden = jnp.concatenate(
        [rows[pl.ds(8 * (t // 3) + t % 3, 16, stride=32), :] for t in range(11)], axis=1
    ).astype(BF)
    term = folded(dot_t(hidden, w_down[...]))
    for i in range(8):
        out[i] = term


def finish(got, residual, out):
    out[...] = (residual[...].astype(F32) + unfolded(summed(got))).astype(BF)


def local(
    tokens,
    attn_gain,
    w_query,
    w_key,
    w_value,
    key_cache,
    value_cache,
    lengths,
    mix_weight,
    head_gain,
    w_out,
    mixer_gain,
    w_gate,
    w_up,
    w_down,
):
    tile = pltpu.VMEM((128, 128), F32)
    wide = pltpu.VMEM((512, 128), F32)
    sent, keys, values, limit, owner, share = run(
        project,
        (
            shape(8, 16, 768),
            shape(16, 512, 128),
            shape(16, 512, 128),
            shape(128, 128, kind=jnp.int32),
            shape(128, 128, kind=jnp.int32),
            shape(8, 128, kind=F32),
        ),
        (
            tokens,
            attn_gain[None],
            w_query,
            w_key,
            w_value,
            lengths,
            mix_weight,
            key_cache.reshape(16, 512, 128),
            value_cache.reshape(16, 512, 128),
        ),
        specs=[HBM] * 9,
        scratch=[
            pltpu.VMEM((16, 64), BF),
            pltpu.VMEM((1, 64), F32),
            pltpu.VMEM((64, 512), BF),
            pltpu.VMEM((64, 512), BF),
            pltpu.VMEM((64, 512), BF),
            pltpu.SMEM((16,), jnp.int32),
            pltpu.SMEM((4,), F32),
            pltpu.SemaphoreType.DMA((9,)),
        ],
    )
    sent = run(relay, shape(8, 16, 768), (exchange(sent, "y"),))
    sent = run(
        attend,
        shape(8, 136, 128),
        (exchange(sent, "z"), keys, values, limit, owner),
        scratch=[tile, tile, tile, pltpu.VMEM((128, 512), F32), tile],
    )
    sent = run(merge, shape(8, 136, 128), (exchange(sent, "y"),))
    sent = run(
        mix,
        shape(8, 8, 128),
        (exchange(sent, "z"), share, head_gain[None], w_out.T),
        scratch=[tile],
    )
    sent, residual = run(
        widen,
        (shape(512, 128), shape(16, 64)),
        (exchange(sent, "tp"), tokens, mixer_gain[None], w_gate, w_up),
        scratch=[wide],
    )
    sent = run(activate, shape(64, 8, 128), (exchange(sent.reshape(64, 8, 128), KV),))
    sent = run(
        narrow, shape(8, 8, 128), (exchange(sent, KV).reshape(512, 128), w_down.T), scratch=[wide]
    )
    return run(finish, jax.ShapeDtypeStruct((16, 64), BF), (exchange(sent, "tp"), residual))


def solution(mesh):
    finer = Mesh(mesh.devices.reshape(8, 8, mesh.shape["tp"]), ("z", "y", "tp"))
    return jax.shard_map(
        local,
        mesh=finer,
        in_specs=(
            P(None, KV),
            P(KV),
            P(KV, "tp"),
            P(KV, "tp"),
            P(KV, "tp"),
            P(None, KV, "tp", None),
            P(None, KV, "tp", None),
            P(),
            P("tp"),
            P(),
            P("tp", KV),
            P(KV),
            P(KV, "tp"),
            P(KV, "tp"),
            P("tp", KV),
        ),
        out_specs=P(None, KV),
        check_vma=False,
    )
```

```python
import jax
import jax.numpy as jnp
from jax import lax
from jax.experimental import pallas as pl
from jax.experimental.pallas import tpu as pltpu
from jax.sharding import Mesh
from jax.sharding import PartitionSpec as P

KV = ("z", "y")
EPS = 1e-06
FLOOR_SCORE = -1e30
BF = jnp.bfloat16
F32 = jnp.float32
VMEM = pl.BlockSpec(memory_space=pltpu.VMEM)
HBM = pl.BlockSpec(memory_space=pltpu.HBM)
INTERPRET = False


def run(kernel, outs, args, specs=None, scratch=(), grant=4):
    single = not isinstance(outs, (list, tuple))
    specs = specs or [VMEM] * len(args)
    if not INTERPRET:
        args = [
            pltpu.with_memory_space_constraint(a, s.memory_space) for a, s in zip(args, specs)
        ]
    return pl.pallas_call(
        kernel,
        out_shape=outs,
        in_specs=specs,
        out_specs=VMEM if single else [VMEM] * len(outs),
        scratch_shapes=scratch,
        compiler_params=pltpu.CompilerParams(vmem_limit_bytes=grant << 20),
        interpret=INTERPRET,
    )(*args)


def shape(*dims, kind=BF):
    return jax.ShapeDtypeStruct(dims, kind) if INTERPRET else pltpu.VMEM(dims, kind)


def exchange(array, axis):
    return lax.all_to_all(array, axis, 0, 0, tiled=True)


def dot(left, right):
    return jnp.dot(left, right, preferred_element_type=F32)


def dot_t(left, right):
    return lax.dot_general(left, right, (((1,), (1,)), ((), ())), preferred_element_type=F32)


def rounded(array):
    return array.astype(BF).astype(F32)


def summed(ref):
    total = ref[0].astype(F32)
    for i in range(1, ref.shape[0]):
        total = total + ref[i].astype(F32)
    return total


def folded(term):
    return jnp.concatenate([term[0:8], term[8:16]], axis=1).astype(BF)


def unfolded(term):
    return jnp.concatenate([term[:, 0:64], term[:, 64:128]], axis=0)


def iota(shape_, dim):
    return lax.broadcasted_iota(jnp.int32, shape_, dim)


def project(
    tokens, gain, w_query, w_key, w_value, lengths, weight, keys, values,
    out, keys_out, values_out, limit, owner, share,
    tokens_in, gain_in, query_in, key_in, value_in, lengths_in, weight_in, sems,
):
    pairs = (
        (tokens, tokens_in),
        (gain, gain_in),
        (w_query, query_in),
        (w_key, key_in),
        (w_value, value_in),
        (lengths, lengths_in),
        (weight, weight_in),
        (keys, keys_out),
        (values, values_out),
    )
    copies = [pltpu.make_async_copy(a, b, sems.at[i]) for i, (a, b) in enumerate(pairs)]
    for copy in copies:
        copy.start()
    for copy in copies[:5]:
        copy.wait()
    x = tokens_in[...].astype(F32)
    scaled = (x * gain_in[...]).astype(BF)
    query = dot(scaled, query_in[...]).astype(BF)
    key = dot(scaled, key_in[...])
    value = dot(scaled, value_in[...])
    squares = jnp.broadcast_to(jnp.sum(x * x, axis=1, keepdims=True), (16, 128)).astype(BF)
    for y in range(8):
        rows = slice(8 * (y // 4), 8 * (y // 4) + 8)
        lanes = slice(128 * (y % 4), 128 * (y % 4) + 128)
        out[y, :, 0:512] = query
        out[y, :, 512:640] = jnp.concatenate([key[rows, lanes], value[rows, lanes]], axis=0).astype(BF)
        out[y, :, 640:768] = squares
    for copy in copies[5:7]:
        copy.wait()
    z, y = lax.axis_index("z"), lax.axis_index("y")
    half, head = y // 4, y % 4
    start = (z * 8 + y) * 128
    row_head = iota((8, 128), 0) >> 1
    same_head = (iota((8, 128), 1) & 3) == row_head
    for b in range(16):
        at = slice(8 * b, 8 * b + 8)
        limit[at, :] = jnp.where(same_head, lengths_in[b] - start, 0)
        mine = jnp.logical_and(z == 0, half == b // 8)
        owner[at, :] = jnp.where(jnp.logical_and(mine, row_head == head), 1, 0)
    lane_head = (iota((8, 128), 1) >> 1) & 3
    low = jnp.where(lane_head == 0, weight_in[0], weight_in[1])
    high = jnp.where(lane_head == 2, weight_in[2], weight_in[3])
    share[...] = jnp.where(lane_head < 2, low, high)
    for copy in copies[7:]:
        copy.wait()


def relay(got, out):
    total = summed(got).astype(BF)
    for i in range(8):
        out[i] = total


def attend(got, keys, values, limit, owner, out, rows_q, rows_k, rows_v, scores, acc):
    total = summed(got)
    inverse = lax.rsqrt(total[:, 640:768] / 4096 + EPS)
    first = iota((16, 128), 1) < 64
    for h in range(4):
        query = rounded(inverse * total[:, 128 * h : 128 * h + 128])
        rows_q[pl.ds(2 * h, 16, stride=8), :] = jnp.where(first, query, 0.0)
        rows_q[pl.ds(2 * h + 1, 16, stride=8), :] = jnp.where(first, 0.0, query)
    for b in range(16):
        at = slice(8 * b, 8 * b + 8)
        scores[at, :] = dot_t(rows_q[at, :].astype(BF), keys[b])
    for part in range(2):
        scale = inverse[8 * part : 8 * part + 8]
        key_new = rounded(scale * total[0:8, 512:640])
        value_new = rounded(scale * total[8:16, 512:640])
        for i in range(8):
            at = pl.ds(64 * part + i, 8, stride=8)
            rows_k[at, :] = key_new
            rows_v[at, :] = value_new
    owned = owner[...] > 0
    own = jnp.sum(rows_q[...] * rows_k[...], axis=1, keepdims=True) * 0.125
    own = jnp.where(owned, own, FLOOR_SCORE)
    lane = iota((128, 128), 1)
    tiles, seen = [], []
    peak = own
    for t in range(4):
        visible = (lane + 128 * t) >> 2 < limit[...]
        tile = jnp.where(visible, scores[:, 128 * t : 128 * t + 128] * 0.125, FLOOR_SCORE)
        tiles.append(tile)
        seen.append(visible)
        peak = jnp.maximum(peak, tile)
    peak = jnp.max(peak, axis=1, keepdims=True)
    peak_hi = rounded(peak)
    peak_lo = rounded(peak - peak_hi)
    base = peak_hi + peak_lo
    weights = [jnp.where(v, jnp.exp(t - base), 0.0) for t, v in zip(tiles, seen)]
    own_weight = jnp.where(owned, jnp.exp(own - base), 0.0)
    totals = jnp.sum(weights[0] + weights[1] + weights[2] + weights[3], axis=1, keepdims=True)
    totals = totals + own_weight
    weights = jnp.concatenate(weights, axis=1).astype(BF)
    for b in range(16):
        at = slice(8 * b, 8 * b + 8)
        acc[at, :] = dot(weights[at, :], values[b])
    body = (acc[...] + rounded(own_weight) * rows_v[...]).T.astype(BF)
    totals_hi = rounded(totals)
    stat = jnp.where(
        lane == 0,
        peak_hi,
        jnp.where(lane == 1, peak_lo, jnp.where(lane == 2, totals_hi, totals - totals_hi)),
    )
    tail = stat.T[0:8].astype(BF)
    for i in range(8):
        out[i, 0:128, :] = body
        out[i, 128:136, :] = tail


def merged(got):
    tails = [got[i, 128:136, :].astype(F32) for i in range(8)]
    peaks = [t[0:1] + t[1:2] for t in tails]
    peak = peaks[0]
    for p in peaks[1:]:
        peak = jnp.maximum(peak, p)
    totals = jnp.zeros_like(peak)
    values = jnp.zeros((128, 128), F32)
    for i in range(8):
        scale = jnp.exp(peaks[i] - peak)
        totals = totals + scale * (tails[i][2:3] + tails[i][3:4])
        values = values + scale * got[i, 0:128, :].astype(F32)
    return peak, totals, values


def merge(got, out):
    peak, totals, values = merged(got)
    peak_hi, totals_hi = rounded(peak), rounded(totals)
    row = iota((8, 128), 0)
    tail = jnp.where(
        row == 0,
        peak_hi,
        jnp.where(row == 1, peak - peak_hi, jnp.where(row == 2, totals_hi, totals - totals_hi)),
    ).astype(BF)
    body = values.astype(BF)
    for i in range(8):
        out[i, 0:128, :] = body
        out[i, 128:136, :] = tail


def mix(got, share, head_gain, w_out, out, rows):
    _, totals, values = merged(got)
    ratio = values / totals
    mixture = ratio - share[0:1] * pltpu.roll(ratio, 127, 1)
    scale = lax.rsqrt(jnp.mean(mixture * mixture, axis=0, keepdims=True) + EPS)
    rows[...] = (mixture * scale).T * head_gain[...]
    attended = jnp.concatenate(
        [rows[pl.ds(2 * h, 16, stride=8), :] for h in range(4)], axis=1
    ).astype(BF)
    term = folded(dot_t(attended, w_out[...]))
    for i in range(8):
        out[i] = term


def widen(got, tokens, gain, w_gate, w_up, out, residual_out, rows):
    residual = (tokens[...].astype(F32) + unfolded(summed(got))).astype(BF)
    residual_out[...] = residual
    x = residual.astype(F32)
    scaled = (x * gain[...]).astype(BF)
    squares = jnp.broadcast_to(jnp.sum(x * x, axis=1, keepdims=True), (16, 128))
    for first, product in ((0, dot(scaled, w_gate[...])), (24, dot(scaled, w_up[...]))):
        for t in range(12):
            tile = product[:, 128 * t : 128 * t + 128] if t < 11 else squares
            rows[pl.ds(first + 2 * t, 8, stride=48), :] = tile[0:8]
            rows[pl.ds(first + 2 * t + 1, 8, stride=48), :] = tile[8:16]
    out[...] = rows[...].astype(BF)


def activate(got, out):
    total = summed(got)
    squares = jnp.where((iota((24, 128), 0) & 1) == 0, total[22:23], total[23:24])
    inverse = lax.rsqrt(squares / 4096 + EPS)
    gate = inverse * total[0:24]
    up = inverse * total[24:48]
    hidden = (gate / (1.0 + jnp.exp(-gate)) * up).astype(BF)
    for i in range(8):
        out[i] = hidden


def narrow(got, w_down, out, rows):
    rows[...] = got[...].astype(F32)
    halves = [
        jnp.concatenate([rows[pl.ds(2 * t + i, 8, stride=24), :] for t in range(11)], axis=1)
        for i in range(2)
    ]
    hidden = jnp.concatenate(halves, axis=0).astype(BF)
    term = folded(dot_t(hidden, w_down[...]))
    for i in range(8):
        out[i] = term


def finish(got, residual, out):
    out[...] = (residual[...].astype(F32) + unfolded(summed(got))).astype(BF)


def local(
    tokens,
    attn_gain,
    w_query,
    w_key,
    w_value,
    key_cache,
    value_cache,
    lengths,
    mix_weight,
    head_gain,
    w_out,
    mixer_gain,
    w_gate,
    w_up,
    w_down,
):
    tile = pltpu.VMEM((128, 128), F32)
    sent, keys, values, limit, owner, share = run(
        project,
        (
            shape(8, 16, 768),
            shape(16, 512, 128),
            shape(16, 512, 128),
            shape(128, 128, kind=jnp.int32),
            shape(128, 128, kind=jnp.int32),
            shape(8, 128, kind=F32),
        ),
        (
            tokens,
            attn_gain[None],
            w_query,
            w_key,
            w_value,
            lengths,
            mix_weight,
            key_cache.reshape(16, 512, 128),
            value_cache.reshape(16, 512, 128),
        ),
        specs=[HBM] * 9,
        scratch=[
            pltpu.VMEM((16, 64), BF),
            pltpu.VMEM((1, 64), F32),
            pltpu.VMEM((64, 512), BF),
            pltpu.VMEM((64, 512), BF),
            pltpu.VMEM((64, 512), BF),
            pltpu.SMEM((16,), jnp.int32),
            pltpu.SMEM((4,), F32),
            pltpu.SemaphoreType.DMA((9,)),
        ],
    )
    sent = run(relay, shape(8, 16, 768), (exchange(sent, "y"),))
    sent = run(
        attend,
        shape(8, 136, 128),
        (exchange(sent, "z"), keys, values, limit, owner),
        scratch=[tile, tile, tile, pltpu.VMEM((128, 512), F32), tile],
    )
    sent = run(merge, shape(8, 136, 128), (exchange(sent, "y"),))
    sent = run(
        mix,
        shape(8, 8, 128),
        (exchange(sent, "z"), share, head_gain[None], w_out.T),
        scratch=[tile],
    )
    sent, residual = run(
        widen,
        (shape(384, 128), shape(16, 64)),
        (exchange(sent, "tp"), tokens, mixer_gain[None], w_gate, w_up),
        scratch=[pltpu.VMEM((384, 128), F32)],
    )
    sent = run(relay, shape(8, 48, 128), (exchange(sent.reshape(8, 48, 128), "y"),))
    sent = run(activate, shape(8, 24, 128), (exchange(sent, "z"),))
    sent = run(
        narrow,
        shape(8, 8, 128),
        (exchange(sent, "y").reshape(192, 128), w_down.T),
        scratch=[pltpu.VMEM((192, 128), F32)],
    )
    return run(finish, jax.ShapeDtypeStruct((16, 64), BF), (exchange(sent, "tp"), residual))


def solution(mesh):
    finer = Mesh(mesh.devices.reshape(8, 8, mesh.shape["tp"]), ("z", "y", "tp"))
    return jax.shard_map(
        local,
        mesh=finer,
        in_specs=(
            P(None, KV),
            P(KV),
            P(KV, "tp"),
            P(KV, "tp"),
            P(KV, "tp"),
            P(None, KV, "tp", None),
            P(None, KV, "tp", None),
            P(),
            P("tp"),
            P(),
            P("tp", KV),
            P(KV),
            P(KV, "tp"),
            P(KV, "tp"),
            P("tp", KV),
        ),
        out_specs=P(None, KV),
        check_vma=False,
    )
```

```python
import jax
import jax.numpy as jnp
from jax import lax
from jax.experimental import pallas as pl
from jax.experimental.pallas import tpu as pltpu
from jax.sharding import Mesh
from jax.sharding import PartitionSpec as P

KV = ("z", "y")
EPS = 1e-06
FLOOR_SCORE = -1e30
BF = jnp.bfloat16
F32 = jnp.float32
VMEM = pl.BlockSpec(memory_space=pltpu.VMEM)
HBM = pl.BlockSpec(memory_space=pltpu.HBM)
INTERPRET = False


def run(kernel, outs, args, specs=None, scratch=(), grant=4):
    single = not isinstance(outs, (list, tuple))
    specs = specs or [VMEM] * len(args)
    if not INTERPRET:
        args = [
            pltpu.with_memory_space_constraint(a, s.memory_space) for a, s in zip(args, specs)
        ]
    return pl.pallas_call(
        kernel,
        out_shape=outs,
        in_specs=specs,
        out_specs=VMEM if single else [VMEM] * len(outs),
        scratch_shapes=scratch,
        compiler_params=pltpu.CompilerParams(vmem_limit_bytes=grant << 20),
        interpret=INTERPRET,
    )(*args)


def shape(*dims, kind=BF):
    return jax.ShapeDtypeStruct(dims, kind) if INTERPRET else pltpu.VMEM(dims, kind)


def exchange(array, axis):
    return lax.all_to_all(array, axis, 0, 0, tiled=True)


def dot(left, right):
    return jnp.dot(left, right, preferred_element_type=F32)


def dot_t(left, right):
    return lax.dot_general(left, right, (((1,), (1,)), ((), ())), preferred_element_type=F32)


def rounded(array):
    return array.astype(BF).astype(F32)


def summed(ref):
    total = ref[0].astype(F32)
    for i in range(1, ref.shape[0]):
        total = total + ref[i].astype(F32)
    return total


def folded(term):
    return jnp.concatenate([term[0:8], term[8:16]], axis=1).astype(BF)


def unfolded(term):
    return jnp.concatenate([term[:, 0:64], term[:, 64:128]], axis=0)


def iota(shape_, dim):
    return lax.broadcasted_iota(jnp.int32, shape_, dim)


def as_row(column):
    here = iota((16, 128), 0) == iota((16, 128), 1)
    return jnp.sum(jnp.where(here, column, 0.0), axis=0, keepdims=True)


def as_column(row):
    here = iota((16, 128), 0) == iota((16, 128), 1)
    return jnp.sum(jnp.where(here, row, 0.0), axis=1, keepdims=True)


def project(
    tokens, gain, w_query, w_key, w_value, lengths, weight, keys, values,
    out, keys_out, values_out, limit, owner, picked, share,
    tokens_in, gain_in, query_in, key_in, value_in, lengths_in, weight_in, sems, live_sems,
):
    pairs = (
        (lengths, lengths_in),
        (tokens, tokens_in),
        (gain, gain_in),
        (w_query, query_in),
        (w_key, key_in),
        (w_value, value_in),
        (weight, weight_in),
    )
    copies = [pltpu.make_async_copy(a, b, sems.at[i]) for i, (a, b) in enumerate(pairs)]
    for copy in copies:
        copy.start()
    z, y = lax.axis_index("z"), lax.axis_index("y")
    half, head = y // 4, y % 4
    start = (z * 8 + y) * 128
    copies[0].wait()

    def cache_copies(b):
        return (
            pltpu.make_async_copy(keys.at[b], keys_out.at[b], live_sems.at[0, b]),
            pltpu.make_async_copy(values.at[b], values_out.at[b], live_sems.at[1, b]),
        )

    for b in range(16):

        @pl.when(lengths_in[b] > start)
        def _(b=b):
            for copy in cache_copies(b):
                copy.start()

    for copy in copies[1:6]:
        copy.wait()
    x = tokens_in[...].astype(F32)
    scaled = (x * gain_in[...]).astype(BF)
    query = dot(scaled, query_in[...]).astype(BF)
    key = dot(scaled, key_in[...])
    value = dot(scaled, value_in[...])
    squares = as_row(jnp.sum(x * x, axis=1, keepdims=True))
    squares = jnp.broadcast_to(squares, (8, 128)).astype(BF)
    for i in range(8):
        rows = slice(8 * (i // 4), 8 * (i // 4) + 8)
        lanes = slice(128 * (i % 4), 128 * (i % 4) + 128)
        for h in range(4):
            out[i, 16 * h : 16 * h + 16, :] = query[:, 128 * h : 128 * h + 128]
        out[i, 64:80, :] = jnp.concatenate([key[rows, lanes], value[rows, lanes]], axis=0).astype(BF)
        out[i, 80:88, :] = squares
    copies[6].wait()
    row_head = iota((8, 128), 0) >> 1
    same_head = (iota((8, 128), 1) & 3) == row_head
    mine = half * 8 + z
    for b in range(16):
        at = slice(8 * b, 8 * b + 8)
        limit[at, :] = jnp.where(same_head, lengths_in[b] - start, 0)
        owner[at, :] = jnp.where(jnp.logical_and(mine == b, row_head == head), 1, 0)
    picked[...] = jnp.where(iota((16, 128), 0) == mine, 1.0, 0.0)
    lane_head = (iota((8, 128), 1) >> 1) & 3
    low = jnp.where(lane_head == 0, weight_in[0], weight_in[1])
    high = jnp.where(lane_head == 2, weight_in[2], weight_in[3])
    share[...] = jnp.where(lane_head < 2, low, high)
    for b in range(16):
        alive = lengths_in[b] > start

        @pl.when(jnp.logical_not(alive))
        def _(b=b):
            keys_out[b] = jnp.zeros((512, 128), BF)
            values_out[b] = jnp.zeros((512, 128), BF)

        @pl.when(alive)
        def _(b=b):
            for copy in cache_copies(b):
                copy.wait()


def relay(got, out):
    total = summed(got).astype(BF)
    for i in range(8):
        out[i] = total


def relay_query(got, out):
    total = summed(got)
    query = total[0:64].astype(BF)
    row = iota((8, 128), 0)
    for i in range(8):
        out[i, 0:64, :] = query
        key = total[64 + i : 65 + i]
        value = total[72 + i : 73 + i]
        last = jnp.where(row == 0, key, jnp.where(row == 1, value, total[80:81]))
        out[i, 64:72, :] = last.astype(BF)


def attend(got, keys, values, limit, owner, picked, out, rows_q, scores, acc):
    total = summed(got)
    inverse = lax.rsqrt(as_column(total[66:67]) / 4096 + EPS)
    first = iota((16, 128), 1) < 64
    for h in range(4):
        query = rounded(inverse * total[16 * h : 16 * h + 16])
        rows_q[pl.ds(2 * h, 16, stride=8), :] = jnp.where(first, query, 0.0)
        rows_q[pl.ds(2 * h + 1, 16, stride=8), :] = jnp.where(first, 0.0, query)
    for b in range(16):
        at = slice(8 * b, 8 * b + 8)
        scores[at, :] = dot_t(rows_q[at, :].astype(BF), keys[b])
    scale = jnp.sum(inverse * picked[...], axis=0, keepdims=True)
    key_new = rounded(scale * total[64:65])
    value_new = rounded(scale * total[65:66])
    owned = owner[...] > 0
    own = jnp.sum(rows_q[...] * key_new, axis=1, keepdims=True) * 0.125
    own = jnp.where(owned, own, FLOOR_SCORE)
    lane = iota((128, 128), 1)
    tiles, seen = [], []
    peak = own
    for t in range(4):
        visible = (lane + 128 * t) >> 2 < limit[...]
        tile = jnp.where(visible, scores[:, 128 * t : 128 * t + 128] * 0.125, FLOOR_SCORE)
        tiles.append(tile)
        seen.append(visible)
        peak = jnp.maximum(peak, tile)
    peak = jnp.max(peak, axis=1, keepdims=True)
    peak_hi = rounded(peak)
    peak_lo = rounded(peak - peak_hi)
    base = peak_hi + peak_lo
    weights = [jnp.where(v, jnp.exp(t - base), 0.0) for t, v in zip(tiles, seen)]
    own_weight = jnp.where(owned, jnp.exp(own - base), 0.0)
    totals = jnp.sum(weights[0] + weights[1] + weights[2] + weights[3], axis=1, keepdims=True)
    totals = totals + own_weight
    weights = jnp.concatenate(weights, axis=1).astype(BF)
    for b in range(16):
        at = slice(8 * b, 8 * b + 8)
        acc[at, :] = dot(weights[at, :], values[b])
    body = (acc[...] + rounded(own_weight) * value_new).T.astype(BF)
    totals_hi = rounded(totals)
    stat = jnp.where(
        lane == 0,
        peak_hi,
        jnp.where(lane == 1, peak_lo, jnp.where(lane == 2, totals_hi, totals - totals_hi)),
    )
    tail = stat.T[0:8].astype(BF)
    for i in range(8):
        out[i, 0:128, :] = body
        out[i, 128:136, :] = tail


def merged(got):
    tails = [got[i, 128:136, :].astype(F32) for i in range(8)]
    peaks = [t[0:1] + t[1:2] for t in tails]
    peak = peaks[0]
    for p in peaks[1:]:
        peak = jnp.maximum(peak, p)
    totals = jnp.zeros_like(peak)
    values = jnp.zeros((128, 128), F32)
    for i in range(8):
        scale = jnp.exp(peaks[i] - peak)
        totals = totals + scale * (tails[i][2:3] + tails[i][3:4])
        values = values + scale * got[i, 0:128, :].astype(F32)
    return peak, totals, values


def merge(got, out):
    peak, totals, values = merged(got)
    peak_hi, totals_hi = rounded(peak), rounded(totals)
    row = iota((8, 128), 0)
    tail = jnp.where(
        row == 0,
        peak_hi,
        jnp.where(row == 1, peak - peak_hi, jnp.where(row == 2, totals_hi, totals - totals_hi)),
    ).astype(BF)
    body = values.astype(BF)
    for i in range(8):
        out[i, 0:128, :] = body
        out[i, 128:136, :] = tail


def mix(got, share, head_gain, w_out, out, rows):
    _, totals, values = merged(got)
    ratio = values / totals
    mixture = ratio - share[0:1] * pltpu.roll(ratio, 127, 1)
    scale = lax.rsqrt(jnp.mean(mixture * mixture, axis=0, keepdims=True) + EPS)
    rows[...] = (mixture * scale).T * head_gain[...]
    attended = jnp.concatenate(
        [rows[pl.ds(2 * h, 16, stride=8), :] for h in range(4)], axis=1
    ).astype(BF)
    term = folded(dot_t(attended, w_out[...]))
    for i in range(8):
        out[i] = term


def widen(got, tokens, gain, w_gate, w_up, out, residual_out, rows):
    residual = (tokens[...].astype(F32) + unfolded(summed(got))).astype(BF)
    residual_out[...] = residual
    x = residual.astype(F32)
    scaled = (x * gain[...]).astype(BF)
    squares = jnp.broadcast_to(jnp.sum(x * x, axis=1, keepdims=True), (16, 128))
    for first, product in ((0, dot(scaled, w_gate[...])), (24, dot(scaled, w_up[...]))):
        for t in range(12):
            tile = product[:, 128 * t : 128 * t + 128] if t < 11 else squares
            rows[pl.ds(first + 2 * t, 8, stride=48), :] = tile[0:8]
            rows[pl.ds(first + 2 * t + 1, 8, stride=48), :] = tile[8:16]
    out[...] = rows[...].astype(BF)


def activate(got, out):
    total = summed(got)
    squares = jnp.where((iota((24, 128), 0) & 1) == 0, total[22:23], total[23:24])
    inverse = lax.rsqrt(squares / 4096 + EPS)
    gate = inverse * total[0:24]
    up = inverse * total[24:48]
    hidden = (gate / (1.0 + jnp.exp(-gate)) * up).astype(BF)
    for i in range(8):
        out[i] = hidden


def narrow(got, w_down, out, rows):
    rows[...] = got[...].astype(F32)
    halves = [
        jnp.concatenate([rows[pl.ds(2 * t + i, 8, stride=24), :] for t in range(11)], axis=1)
        for i in range(2)
    ]
    hidden = jnp.concatenate(halves, axis=0).astype(BF)
    term = folded(dot_t(hidden, w_down[...]))
    for i in range(8):
        out[i] = term


def finish(got, residual, out):
    out[...] = (residual[...].astype(F32) + unfolded(summed(got))).astype(BF)


def local(
    tokens,
    attn_gain,
    w_query,
    w_key,
    w_value,
    key_cache,
    value_cache,
    lengths,
    mix_weight,
    head_gain,
    w_out,
    mixer_gain,
    w_gate,
    w_up,
    w_down,
):
    tile = pltpu.VMEM((128, 128), F32)
    sent, keys, values, limit, owner, picked, share = run(
        project,
        (
            shape(8, 88, 128),
            shape(16, 512, 128),
            shape(16, 512, 128),
            shape(128, 128, kind=jnp.int32),
            shape(128, 128, kind=jnp.int32),
            shape(16, 128, kind=F32),
            shape(8, 128, kind=F32),
        ),
        (
            tokens,
            attn_gain[None],
            w_query,
            w_key,
            w_value,
            lengths,
            mix_weight,
            key_cache.reshape(16, 512, 128),
            value_cache.reshape(16, 512, 128),
        ),
        specs=[HBM] * 9,
        scratch=[
            pltpu.VMEM((16, 64), BF),
            pltpu.VMEM((1, 64), F32),
            pltpu.VMEM((64, 512), BF),
            pltpu.VMEM((64, 512), BF),
            pltpu.VMEM((64, 512), BF),
            pltpu.SMEM((16,), jnp.int32),
            pltpu.SMEM((4,), F32),
            pltpu.SemaphoreType.DMA((7,)),
            pltpu.SemaphoreType.DMA((2, 16)),
        ],
    )
    sent = run(relay_query, shape(8, 72, 128), (exchange(sent, "y"),))
    sent = run(
        attend,
        shape(8, 136, 128),
        (exchange(sent, "z"), keys, values, limit, owner, picked),
        scratch=[tile, pltpu.VMEM((128, 512), F32), tile],
    )
    sent = run(merge, shape(8, 136, 128), (exchange(sent, "y"),))
    sent = run(
        mix,
        shape(8, 8, 128),
        (exchange(sent, "z"), share, head_gain[None], w_out.T),
        scratch=[tile],
    )
    sent, residual = run(
        widen,
        (shape(384, 128), shape(16, 64)),
        (exchange(sent, "tp"), tokens, mixer_gain[None], w_gate, w_up),
        scratch=[pltpu.VMEM((384, 128), F32)],
    )
    sent = run(relay, shape(8, 48, 128), (exchange(sent.reshape(8, 48, 128), "y"),))
    sent = run(activate, shape(8, 24, 128), (exchange(sent, "z"),))
    sent = run(
        narrow,
        shape(8, 8, 128),
        (exchange(sent, "y").reshape(192, 128), w_down.T),
        scratch=[pltpu.VMEM((192, 128), F32)],
    )
    return run(finish, jax.ShapeDtypeStruct((16, 64), BF), (exchange(sent, "tp"), residual))


def solution(mesh):
    finer = Mesh(mesh.devices.reshape(8, 8, mesh.shape["tp"]), ("z", "y", "tp"))
    return jax.shard_map(
        local,
        mesh=finer,
        in_specs=(
            P(None, KV),
            P(KV),
            P(KV, "tp"),
            P(KV, "tp"),
            P(KV, "tp"),
            P(None, KV, "tp", None),
            P(None, KV, "tp", None),
            P(),
            P("tp"),
            P(),
            P("tp", KV),
            P(KV),
            P(KV, "tp"),
            P(KV, "tp"),
            P("tp", KV),
        ),
        out_specs=P(None, KV),
        check_vma=False,
    )
```

```python
import jax
import jax.numpy as jnp
from jax import lax
from jax.experimental import pallas as pl
from jax.experimental.pallas import tpu as pltpu
from jax.sharding import Mesh
from jax.sharding import PartitionSpec as P

KV = ("z", "y")
EPS = 1e-06
FLOOR_SCORE = -1e30
BF = jnp.bfloat16
F32 = jnp.float32
VMEM = pl.BlockSpec(memory_space=pltpu.VMEM)
HBM = pl.BlockSpec(memory_space=pltpu.HBM)
INTERPRET = False


def run(kernel, outs, args, specs=None, scratch=(), grant=4):
    single = not isinstance(outs, (list, tuple))
    specs = specs or [VMEM] * len(args)
    if not INTERPRET:
        args = [
            pltpu.with_memory_space_constraint(a, s.memory_space) for a, s in zip(args, specs)
        ]
    return pl.pallas_call(
        kernel,
        out_shape=outs,
        in_specs=specs,
        out_specs=VMEM if single else [VMEM] * len(outs),
        scratch_shapes=scratch,
        compiler_params=pltpu.CompilerParams(vmem_limit_bytes=grant << 20),
        interpret=INTERPRET,
    )(*args)


def shape(*dims, kind=BF):
    return jax.ShapeDtypeStruct(dims, kind) if INTERPRET else pltpu.VMEM(dims, kind)


def exchange(array, axis):
    return lax.all_to_all(array, axis, 0, 0, tiled=True)


def dot(left, right):
    return jnp.dot(left, right, preferred_element_type=F32)


def dot_t(left, right):
    return lax.dot_general(left, right, (((1,), (1,)), ((), ())), preferred_element_type=F32)


def rounded(array):
    return array.astype(BF).astype(F32)


def summed(ref):
    total = ref[0].astype(F32)
    for i in range(1, ref.shape[0]):
        total = total + ref[i].astype(F32)
    return total


def folded(term):
    return jnp.concatenate([term[0:8], term[8:16]], axis=1).astype(BF)


def unfolded(term):
    return jnp.concatenate([term[:, 0:64], term[:, 64:128]], axis=0)


def iota(shape_, dim):
    return lax.broadcasted_iota(jnp.int32, shape_, dim)


def as_row(column):
    here = iota((16, 128), 0) == iota((16, 128), 1)
    return jnp.sum(jnp.where(here, column, 0.0), axis=0, keepdims=True)


def as_column(row):
    here = iota((16, 128), 0) == iota((16, 128), 1)
    return jnp.sum(jnp.where(here, row, 0.0), axis=1, keepdims=True)


def project(
    tokens, gain, w_query, w_key, w_value, lengths, weight, keys, values,
    out, keys_out, values_out, limit, owner, picked, share,
    tokens_in, gain_in, query_in, key_in, value_in, lengths_in, weight_in, sems, live_sems,
):
    pairs = (
        (lengths, lengths_in),
        (tokens, tokens_in),
        (gain, gain_in),
        (w_query, query_in),
        (w_key, key_in),
        (w_value, value_in),
        (weight, weight_in),
    )
    copies = [pltpu.make_async_copy(a, b, sems.at[i]) for i, (a, b) in enumerate(pairs)]
    for copy in copies:
        copy.start()
    z, y = lax.axis_index("z"), lax.axis_index("y")
    half, head = y // 4, y % 4
    start = (z * 8 + y) * 128
    keys_out[...] = jnp.zeros((16, 512, 128), BF)
    values_out[...] = jnp.zeros((16, 512, 128), BF)
    mine = half * 8 + z
    row_head = iota((8, 128), 0) >> 1
    same_head = (iota((8, 128), 1) & 3) == row_head
    for b in range(16):
        own_row = jnp.logical_and(mine == b, row_head == head)
        owner[8 * b : 8 * b + 8, :] = jnp.where(own_row, 1, 0)
    picked[...] = jnp.where(iota((16, 128), 0) == mine, 1.0, 0.0)

    def cache_copies(b):
        return (
            pltpu.make_async_copy(keys.at[b], keys_out.at[b], live_sems.at[0, b]),
            pltpu.make_async_copy(values.at[b], values_out.at[b], live_sems.at[1, b]),
        )

    copies[0].wait()
    for b in range(16):

        @pl.when(lengths_in[b] > start)
        def _(b=b):
            for copy in cache_copies(b):
                copy.start()

    for copy in copies[1:6]:
        copy.wait()
    x = tokens_in[...].astype(F32)
    scaled = (x * gain_in[...]).astype(BF)
    query = dot(scaled, query_in[...]).astype(BF)
    key = dot(scaled, key_in[...])
    value = dot(scaled, value_in[...])
    squares = as_row(jnp.sum(x * x, axis=1, keepdims=True))
    squares = jnp.broadcast_to(squares, (8, 128)).astype(BF)
    for i in range(8):
        rows = slice(8 * (i // 4), 8 * (i // 4) + 8)
        lanes = slice(128 * (i % 4), 128 * (i % 4) + 128)
        for h in range(4):
            out[i, 16 * h : 16 * h + 16, :] = query[:, 128 * h : 128 * h + 128]
        out[i, 64:80, :] = jnp.concatenate([key[rows, lanes], value[rows, lanes]], axis=0).astype(BF)
        out[i, 80:88, :] = squares
    copies[6].wait()
    for b in range(16):
        limit[8 * b : 8 * b + 8, :] = jnp.where(same_head, lengths_in[b] - start, 0)
    lane_head = (iota((8, 128), 1) >> 1) & 3
    low = jnp.where(lane_head == 0, weight_in[0], weight_in[1])
    high = jnp.where(lane_head == 2, weight_in[2], weight_in[3])
    share[...] = jnp.where(lane_head < 2, low, high)
    for b in range(16):

        @pl.when(lengths_in[b] > start)
        def _(b=b):
            for copy in cache_copies(b):
                copy.wait()


def relay(got, out):
    total = summed(got).astype(BF)
    for i in range(8):
        out[i] = total


def relay_query(got, out):
    total = summed(got)
    query = total[0:64].astype(BF)
    row = iota((8, 128), 0)
    for i in range(8):
        out[i, 0:64, :] = query
        key = total[64 + i : 65 + i]
        value = total[72 + i : 73 + i]
        last = jnp.where(row == 0, key, jnp.where(row == 1, value, total[80:81]))
        out[i, 64:72, :] = last.astype(BF)


def attend(got, keys, values, limit, owner, picked, out, rows_q, scores, acc):
    total = summed(got)
    inverse = lax.rsqrt(as_column(total[66:67]) / 4096 + EPS)
    first = iota((16, 128), 1) < 64
    for h in range(4):
        query = rounded(inverse * total[16 * h : 16 * h + 16])
        rows_q[pl.ds(2 * h, 16, stride=8), :] = jnp.where(first, query, 0.0)
        rows_q[pl.ds(2 * h + 1, 16, stride=8), :] = jnp.where(first, 0.0, query)
    for b in range(16):
        at = slice(8 * b, 8 * b + 8)
        scores[at, :] = dot_t(rows_q[at, :].astype(BF), keys[b])
    scale = jnp.sum(inverse * picked[...], axis=0, keepdims=True)
    key_new = rounded(scale * total[64:65])
    value_new = rounded(scale * total[65:66])
    owned = owner[...] > 0
    own = jnp.sum(rows_q[...] * key_new, axis=1, keepdims=True) * 0.125
    own = jnp.where(owned, own, FLOOR_SCORE)
    lane = iota((128, 128), 1)
    tiles, seen = [], []
    peak = own
    for t in range(4):
        visible = (lane + 128 * t) >> 2 < limit[...]
        tile = jnp.where(visible, scores[:, 128 * t : 128 * t + 128] * 0.125, FLOOR_SCORE)
        tiles.append(tile)
        seen.append(visible)
        peak = jnp.maximum(peak, tile)
    peak = jnp.max(peak, axis=1, keepdims=True)
    peak_hi = rounded(peak)
    peak_lo = rounded(peak - peak_hi)
    base = peak_hi + peak_lo
    weights = [jnp.where(v, jnp.exp(t - base), 0.0) for t, v in zip(tiles, seen)]
    own_weight = jnp.where(owned, jnp.exp(own - base), 0.0)
    totals = jnp.sum(weights[0] + weights[1] + weights[2] + weights[3], axis=1, keepdims=True)
    totals = totals + own_weight
    weights = jnp.concatenate(weights, axis=1).astype(BF)
    for b in range(16):
        at = slice(8 * b, 8 * b + 8)
        acc[at, :] = dot(weights[at, :], values[b])
    body = (acc[...] + rounded(own_weight) * value_new).T.astype(BF)
    totals_hi = rounded(totals)
    stat = jnp.where(
        lane == 0,
        peak_hi,
        jnp.where(lane == 1, peak_lo, jnp.where(lane == 2, totals_hi, totals - totals_hi)),
    )
    tail = stat.T[0:8].astype(BF)
    for i in range(8):
        out[i, 0:128, :] = body
        out[i, 128:136, :] = tail


def merged(got):
    tails = [got[i, 128:136, :].astype(F32) for i in range(8)]
    peaks = [t[0:1] + t[1:2] for t in tails]
    peak = peaks[0]
    for p in peaks[1:]:
        peak = jnp.maximum(peak, p)
    totals = jnp.zeros_like(peak)
    values = jnp.zeros((128, 128), F32)
    for i in range(8):
        scale = jnp.exp(peaks[i] - peak)
        totals = totals + scale * (tails[i][2:3] + tails[i][3:4])
        values = values + scale * got[i, 0:128, :].astype(F32)
    return peak, totals, values


def merge(got, out):
    peak, totals, values = merged(got)
    peak_hi, totals_hi = rounded(peak), rounded(totals)
    row = iota((8, 128), 0)
    tail = jnp.where(
        row == 0,
        peak_hi,
        jnp.where(row == 1, peak - peak_hi, jnp.where(row == 2, totals_hi, totals - totals_hi)),
    ).astype(BF)
    body = values.astype(BF)
    for i in range(8):
        out[i, 0:128, :] = body
        out[i, 128:136, :] = tail


def mix(got, share, head_gain, w_out, out, rows):
    _, totals, values = merged(got)
    ratio = values / totals
    mixture = ratio - share[0:1] * pltpu.roll(ratio, 127, 1)
    scale = lax.rsqrt(jnp.mean(mixture * mixture, axis=0, keepdims=True) + EPS)
    rows[...] = (mixture * scale).T * head_gain[...]
    attended = jnp.concatenate(
        [rows[pl.ds(2 * h, 16, stride=8), :] for h in range(4)], axis=1
    ).astype(BF)
    term = folded(dot_t(attended, w_out[...]))
    for i in range(8):
        out[i] = term


def widen(got, tokens, gain, w_gate, w_up, out, residual_out, rows):
    residual = (tokens[...].astype(F32) + unfolded(summed(got))).astype(BF)
    residual_out[...] = residual
    x = residual.astype(F32)
    scaled = (x * gain[...]).astype(BF)
    squares = jnp.broadcast_to(jnp.sum(x * x, axis=1, keepdims=True), (16, 128))
    for first, product in ((0, dot(scaled, w_gate[...])), (24, dot(scaled, w_up[...]))):
        for t in range(12):
            tile = product[:, 128 * t : 128 * t + 128] if t < 11 else squares
            rows[pl.ds(first + 2 * t, 8, stride=48), :] = tile[0:8]
            rows[pl.ds(first + 2 * t + 1, 8, stride=48), :] = tile[8:16]
    out[...] = rows[...].astype(BF)


def activate(got, out):
    total = summed(got)
    squares = jnp.where((iota((24, 128), 0) & 1) == 0, total[22:23], total[23:24])
    inverse = lax.rsqrt(squares / 4096 + EPS)
    gate = inverse * total[0:24]
    up = inverse * total[24:48]
    hidden = (gate / (1.0 + jnp.exp(-gate)) * up).astype(BF)
    for i in range(8):
        out[i] = hidden


def narrow(got, w_down, out, rows):
    rows[...] = got[...].astype(F32)
    halves = [
        jnp.concatenate([rows[pl.ds(2 * t + i, 8, stride=24), :] for t in range(11)], axis=1)
        for i in range(2)
    ]
    hidden = jnp.concatenate(halves, axis=0).astype(BF)
    term = folded(dot_t(hidden, w_down[...]))
    for i in range(8):
        out[i] = term


def finish(got, residual, out):
    out[...] = (residual[...].astype(F32) + unfolded(summed(got))).astype(BF)


def local(
    tokens,
    attn_gain,
    w_query,
    w_key,
    w_value,
    key_cache,
    value_cache,
    lengths,
    mix_weight,
    head_gain,
    w_out,
    mixer_gain,
    w_gate,
    w_up,
    w_down,
):
    tile = pltpu.VMEM((128, 128), F32)
    sent, keys, values, limit, owner, picked, share = run(
        project,
        (
            shape(8, 88, 128),
            shape(16, 512, 128),
            shape(16, 512, 128),
            shape(128, 128, kind=jnp.int32),
            shape(128, 128, kind=jnp.int32),
            shape(16, 128, kind=F32),
            shape(8, 128, kind=F32),
        ),
        (
            tokens,
            attn_gain[None],
            w_query,
            w_key,
            w_value,
            lengths,
            mix_weight,
            key_cache.reshape(16, 512, 128),
            value_cache.reshape(16, 512, 128),
        ),
        specs=[HBM] * 9,
        scratch=[
            pltpu.VMEM((16, 64), BF),
            pltpu.VMEM((1, 64), F32),
            pltpu.VMEM((64, 512), BF),
            pltpu.VMEM((64, 512), BF),
            pltpu.VMEM((64, 512), BF),
            pltpu.SMEM((16,), jnp.int32),
            pltpu.SMEM((4,), F32),
            pltpu.SemaphoreType.DMA((7,)),
            pltpu.SemaphoreType.DMA((2, 16)),
        ],
    )
    sent = run(relay_query, shape(8, 72, 128), (exchange(sent, "y"),))
    sent = run(
        attend,
        shape(8, 136, 128),
        (exchange(sent, "z"), keys, values, limit, owner, picked),
        scratch=[tile, pltpu.VMEM((128, 512), F32), tile],
    )
    sent = run(merge, shape(8, 136, 128), (exchange(sent, "z"),))
    sent = run(
        mix,
        shape(8, 8, 128),
        (exchange(sent, "y"), share, head_gain[None], w_out.T),
        scratch=[tile],
    )
    sent, residual = run(
        widen,
        (shape(384, 128), shape(16, 64)),
        (exchange(sent, "tp"), tokens, mixer_gain[None], w_gate, w_up),
        scratch=[pltpu.VMEM((384, 128), F32)],
    )
    sent = run(relay, shape(8, 48, 128), (exchange(sent.reshape(8, 48, 128), "y"),))
    sent = run(activate, shape(8, 24, 128), (exchange(sent, "z"),))
    sent = run(
        narrow,
        shape(8, 8, 128),
        (exchange(sent, "y").reshape(192, 128), w_down.T),
        scratch=[pltpu.VMEM((192, 128), F32)],
    )
    return run(finish, jax.ShapeDtypeStruct((16, 64), BF), (exchange(sent, "tp"), residual))


def solution(mesh):
    finer = Mesh(mesh.devices.reshape(8, 8, mesh.shape["tp"]), ("z", "y", "tp"))
    return jax.shard_map(
        local,
        mesh=finer,
        in_specs=(
            P(None, KV),
            P(KV),
            P(KV, "tp"),
            P(KV, "tp"),
            P(KV, "tp"),
            P(None, KV, "tp", None),
            P(None, KV, "tp", None),
            P(),
            P("tp"),
            P(),
            P("tp", KV),
            P(KV),
            P(KV, "tp"),
            P(KV, "tp"),
            P("tp", KV),
        ),
        out_specs=P(None, KV),
        check_vma=False,
    )
```

```python
import jax
import jax.numpy as jnp
from jax import lax
from jax.experimental import pallas as pl
from jax.experimental.pallas import tpu as pltpu
from jax.sharding import Mesh
from jax.sharding import PartitionSpec as P

Z = ("z_hi", "z_lo")
KV = ("z_hi", "z_lo", "y")
GATHER = ("z_lo", "y")
EPS = 1e-06
FLOOR_SCORE = -1e30
BF = jnp.bfloat16
F32 = jnp.float32
VMEM = pl.BlockSpec(memory_space=pltpu.VMEM)
HBM = pl.BlockSpec(memory_space=pltpu.HBM)
INTERPRET = False


def run(kernel, outs, args, specs=None, scratch=(), grant=4):
    single = not isinstance(outs, (list, tuple))
    specs = specs or [VMEM] * len(args)
    if not INTERPRET:
        args = [
            pltpu.with_memory_space_constraint(a, s.memory_space) for a, s in zip(args, specs)
        ]
    return pl.pallas_call(
        kernel,
        out_shape=outs,
        in_specs=specs,
        out_specs=VMEM if single else [VMEM] * len(outs),
        scratch_shapes=scratch,
        compiler_params=pltpu.CompilerParams(vmem_limit_bytes=grant << 20),
        interpret=INTERPRET,
    )(*args)


def shape(*dims, kind=BF):
    return jax.ShapeDtypeStruct(dims, kind) if INTERPRET else pltpu.VMEM(dims, kind)


def exchange(array, axis):
    return lax.all_to_all(array, axis, 0, 0, tiled=True)


def dot(left, right):
    return jnp.dot(left, right, preferred_element_type=F32)


def dot_t(left, right):
    return lax.dot_general(left, right, (((1,), (1,)), ((), ())), preferred_element_type=F32)


def rounded(array):
    return array.astype(BF).astype(F32)


def summed(ref):
    total = ref[0].astype(F32)
    for i in range(1, ref.shape[0]):
        total = total + ref[i].astype(F32)
    return total


def folded(term):
    return jnp.concatenate([term[0:8], term[8:16]], axis=1).astype(BF)


def unfolded(term):
    return jnp.concatenate([term[:, 0:64], term[:, 64:128]], axis=0)


def iota(shape_, dim):
    return lax.broadcasted_iota(jnp.int32, shape_, dim)


def as_row(column):
    here = iota((16, 128), 0) == iota((16, 128), 1)
    return jnp.sum(jnp.where(here, column, 0.0), axis=0, keepdims=True)


def as_column(row):
    here = iota((16, 128), 0) == iota((16, 128), 1)
    return jnp.sum(jnp.where(here, row, 0.0), axis=1, keepdims=True)


def project(
    tokens, gain, w_query, w_key, w_value, lengths, weight, keys, values,
    out, keys_out, values_out, limit, owner, picked, share,
    tokens_in, gain_in, query_in, key_in, value_in, lengths_in, weight_in, sems, live_sems,
):
    pairs = (
        (lengths, lengths_in),
        (tokens, tokens_in),
        (gain, gain_in),
        (w_query, query_in),
        (w_key, key_in),
        (w_value, value_in),
        (weight, weight_in),
    )
    copies = [pltpu.make_async_copy(a, b, sems.at[i]) for i, (a, b) in enumerate(pairs)]
    for copy in copies:
        copy.start()
    z, y = lax.axis_index("z_hi") * 2 + lax.axis_index("z_lo"), lax.axis_index("y")
    half, head = y // 4, y % 4
    start = (z * 8 + y) * 128
    keys_out[...] = jnp.zeros((16, 512, 128), BF)
    values_out[...] = jnp.zeros((16, 512, 128), BF)
    mine = half * 8 + z
    row_head = iota((8, 128), 0) >> 1
    same_head = (iota((8, 128), 1) & 3) == row_head
    for b in range(16):
        own_row = jnp.logical_and(mine == b, row_head == head)
        owner[8 * b : 8 * b + 8, :] = jnp.where(own_row, 1, 0)
    picked[...] = jnp.where(iota((16, 128), 0) == mine, 1.0, 0.0)

    def cache_copies(b):
        return (
            pltpu.make_async_copy(keys.at[b], keys_out.at[b], live_sems.at[0, b]),
            pltpu.make_async_copy(values.at[b], values_out.at[b], live_sems.at[1, b]),
        )

    copies[0].wait()
    for b in range(16):

        @pl.when(lengths_in[b] > start)
        def _(b=b):
            for copy in cache_copies(b):
                copy.start()

    for copy in copies[1:6]:
        copy.wait()
    x = tokens_in[...].astype(F32)
    scaled = (x * gain_in[...]).astype(BF)
    query = dot(scaled, query_in[...]).astype(BF)
    key = dot(scaled, key_in[...])
    value = dot(scaled, value_in[...])
    squares = as_row(jnp.sum(x * x, axis=1, keepdims=True))
    squares = jnp.broadcast_to(squares, (8, 128)).astype(BF)
    for i in range(8):
        rows = slice(8 * (i // 4), 8 * (i // 4) + 8)
        lanes = slice(128 * (i % 4), 128 * (i % 4) + 128)
        for h in range(4):
            out[i, 16 * h : 16 * h + 16, :] = query[:, 128 * h : 128 * h + 128]
        out[i, 64:80, :] = jnp.concatenate([key[rows, lanes], value[rows, lanes]], axis=0).astype(BF)
        out[i, 80:88, :] = squares
    copies[6].wait()
    for b in range(16):
        limit[8 * b : 8 * b + 8, :] = jnp.where(same_head, lengths_in[b] - start, 0)
    lane_head = (iota((8, 128), 1) >> 1) & 3
    low = jnp.where(lane_head == 0, weight_in[0], weight_in[1])
    high = jnp.where(lane_head == 2, weight_in[2], weight_in[3])
    share[...] = jnp.where(lane_head < 2, low, high)
    for b in range(16):

        @pl.when(lengths_in[b] > start)
        def _(b=b):
            for copy in cache_copies(b):
                copy.wait()


def relay_query(got, out):
    total = summed(got)
    query = total[0:64].astype(BF)
    row = iota((8, 128), 0)
    for i in range(8):
        out[i, 0:64, :] = query
        key = total[64 + i : 65 + i]
        value = total[72 + i : 73 + i]
        last = jnp.where(row == 0, key, jnp.where(row == 1, value, total[80:81]))
        out[i, 64:72, :] = last.astype(BF)


def attend(got, keys, values, limit, owner, picked, out, rows_q, scores, acc):
    total = summed(got)
    inverse = lax.rsqrt(as_column(total[66:67]) / 4096 + EPS)
    first = iota((16, 128), 1) < 64
    for h in range(4):
        query = rounded(inverse * total[16 * h : 16 * h + 16])
        rows_q[pl.ds(2 * h, 16, stride=8), :] = jnp.where(first, query, 0.0)
        rows_q[pl.ds(2 * h + 1, 16, stride=8), :] = jnp.where(first, 0.0, query)
    for b in range(16):
        at = slice(8 * b, 8 * b + 8)
        scores[at, :] = dot_t(rows_q[at, :].astype(BF), keys[b])
    scale = jnp.sum(inverse * picked[...], axis=0, keepdims=True)
    key_new = rounded(scale * total[64:65])
    value_new = rounded(scale * total[65:66])
    owned = owner[...] > 0
    own = jnp.sum(rows_q[...] * key_new, axis=1, keepdims=True) * 0.125
    own = jnp.where(owned, own, FLOOR_SCORE)
    lane = iota((128, 128), 1)
    tiles, seen = [], []
    peak = own
    for t in range(4):
        visible = (lane + 128 * t) >> 2 < limit[...]
        tile = jnp.where(visible, scores[:, 128 * t : 128 * t + 128] * 0.125, FLOOR_SCORE)
        tiles.append(tile)
        seen.append(visible)
        peak = jnp.maximum(peak, tile)
    peak = jnp.max(peak, axis=1, keepdims=True)
    peak_hi = rounded(peak)
    peak_lo = rounded(peak - peak_hi)
    base = peak_hi + peak_lo
    weights = [jnp.where(v, jnp.exp(t - base), 0.0) for t, v in zip(tiles, seen)]
    own_weight = jnp.where(owned, jnp.exp(own - base), 0.0)
    totals = jnp.sum(weights[0] + weights[1] + weights[2] + weights[3], axis=1, keepdims=True)
    totals = totals + own_weight
    weights = jnp.concatenate(weights, axis=1).astype(BF)
    for b in range(16):
        at = slice(8 * b, 8 * b + 8)
        acc[at, :] = dot(weights[at, :], values[b])
    body = (acc[...] + rounded(own_weight) * value_new).T.astype(BF)
    totals_hi = rounded(totals)
    stat = jnp.where(
        lane == 0,
        peak_hi,
        jnp.where(lane == 1, peak_lo, jnp.where(lane == 2, totals_hi, totals - totals_hi)),
    )
    tail = stat.T[0:8].astype(BF)
    for i in range(8):
        out[i, 0:128, :] = body
        out[i, 128:136, :] = tail


def merged(got):
    tails = [got[i, 128:136, :].astype(F32) for i in range(8)]
    peaks = [t[0:1] + t[1:2] for t in tails]
    peak = peaks[0]
    for p in peaks[1:]:
        peak = jnp.maximum(peak, p)
    totals = jnp.zeros_like(peak)
    values = jnp.zeros((128, 128), F32)
    for i in range(8):
        scale = jnp.exp(peaks[i] - peak)
        totals = totals + scale * (tails[i][2:3] + tails[i][3:4])
        values = values + scale * got[i, 0:128, :].astype(F32)
    return peak, totals, values


def merge(got, out):
    peak, totals, values = merged(got)
    peak_hi, totals_hi = rounded(peak), rounded(totals)
    row = iota((8, 128), 0)
    tail = jnp.where(
        row == 0,
        peak_hi,
        jnp.where(row == 1, peak - peak_hi, jnp.where(row == 2, totals_hi, totals - totals_hi)),
    ).astype(BF)
    body = values.astype(BF)
    for i in range(8):
        out[i, 0:128, :] = body
        out[i, 128:136, :] = tail


def mix(got, share, head_gain, w_out, out, rows):
    _, totals, values = merged(got)
    ratio = values / totals
    mixture = ratio - share[0:1] * pltpu.roll(ratio, 127, 1)
    scale = lax.rsqrt(jnp.mean(mixture * mixture, axis=0, keepdims=True) + EPS)
    rows[...] = (mixture * scale).T * head_gain[...]
    attended = jnp.concatenate(
        [rows[pl.ds(2 * h, 16, stride=8), :] for h in range(4)], axis=1
    ).astype(BF)
    term = folded(dot_t(attended, w_out[...]))
    for i in range(8):
        out[i] = term


def widen(got, tokens, gain, w_gate, w_up, out, residual_out, rows):
    residual = (tokens[...].astype(F32) + unfolded(summed(got))).astype(BF)
    residual_out[...] = residual
    x = residual.astype(F32)
    scaled = (x * gain[...]).astype(BF)
    squares = jnp.broadcast_to(jnp.sum(x * x, axis=1, keepdims=True), (16, 128))
    for first, product in ((0, dot(scaled, w_gate[...])), (12, dot(scaled, w_up[...]))):
        for t in range(12):
            tile = product[:, 128 * t : 128 * t + 128] if t < 11 else squares
            rows[pl.ds(first + t, 16, stride=24), :] = tile
    sent = rows[...].astype(BF)
    for i in range(4):
        out[384 * i : 384 * i + 384, :] = sent


def activate(got, out):
    total = summed(got)
    inverse = lax.rsqrt(total[11:12] / 4096 + EPS)
    gate = inverse * total[0:12]
    up = inverse * total[12:24]
    hidden = gate / (1.0 + jnp.exp(-gate)) * up
    hidden = jnp.concatenate([hidden, jnp.zeros((4, 128), F32)], axis=0).astype(BF)
    for i in range(16):
        out[i] = hidden


def narrow(got, w_down, out, rows):
    rows[...] = got[...].astype(F32)
    hidden = jnp.concatenate([rows[pl.ds(t, 16, stride=16), :] for t in range(11)], axis=1)
    term = folded(dot_t(hidden.astype(BF), w_down[...]))
    for i in range(8):
        out[i] = term


def finish(got, residual, out):
    out[...] = (residual[...].astype(F32) + unfolded(summed(got))).astype(BF)


def local(
    tokens,
    attn_gain,
    w_query,
    w_key,
    w_value,
    key_cache,
    value_cache,
    lengths,
    mix_weight,
    head_gain,
    w_out,
    mixer_gain,
    w_gate,
    w_up,
    w_down,
):
    tile = pltpu.VMEM((128, 128), F32)
    sent, keys, values, limit, owner, picked, share = run(
        project,
        (
            shape(8, 88, 128),
            shape(16, 512, 128),
            shape(16, 512, 128),
            shape(128, 128, kind=jnp.int32),
            shape(128, 128, kind=jnp.int32),
            shape(16, 128, kind=F32),
            shape(8, 128, kind=F32),
        ),
        (
            tokens,
            attn_gain[None],
            w_query,
            w_key,
            w_value,
            lengths,
            mix_weight,
            key_cache.reshape(16, 512, 128),
            value_cache.reshape(16, 512, 128),
        ),
        specs=[HBM] * 9,
        scratch=[
            pltpu.VMEM((16, 64), BF),
            pltpu.VMEM((1, 64), F32),
            pltpu.VMEM((64, 512), BF),
            pltpu.VMEM((64, 512), BF),
            pltpu.VMEM((64, 512), BF),
            pltpu.SMEM((16,), jnp.int32),
            pltpu.SMEM((4,), F32),
            pltpu.SemaphoreType.DMA((7,)),
            pltpu.SemaphoreType.DMA((2, 16)),
        ],
    )
    sent = run(relay_query, shape(8, 72, 128), (exchange(sent, "y"),))
    sent = run(
        attend,
        shape(8, 136, 128),
        (exchange(sent, Z), keys, values, limit, owner, picked),
        scratch=[tile, pltpu.VMEM((128, 512), F32), tile],
    )
    sent = run(merge, shape(8, 136, 128), (exchange(sent, Z),))
    sent = run(
        mix,
        shape(8, 8, 128),
        (exchange(sent, "y"), share, head_gain[None], w_out.T),
        scratch=[tile],
    )
    sent, residual = run(
        widen,
        (shape(1536, 128), shape(16, 64)),
        (exchange(sent, "tp"), tokens, mixer_gain[None], w_gate, w_up),
        scratch=[pltpu.VMEM((384, 128), F32)],
    )
    sent = run(activate, shape(16, 16, 128), (exchange(sent.reshape(64, 24, 128), KV),))
    sent = run(
        narrow,
        shape(8, 8, 128),
        (exchange(sent, GATHER).reshape(256, 128), w_down.T),
        scratch=[pltpu.VMEM((256, 128), F32)],
    )
    return run(finish, jax.ShapeDtypeStruct((16, 64), BF), (exchange(sent, "tp"), residual))


def solution(mesh):
    finer = Mesh(mesh.devices.reshape(4, 2, 8, mesh.shape["tp"]), (*KV, "tp"))
    return jax.shard_map(
        local,
        mesh=finer,
        in_specs=(
            P(None, KV),
            P(KV),
            P(KV, "tp"),
            P(KV, "tp"),
            P(KV, "tp"),
            P(None, KV, "tp", None),
            P(None, KV, "tp", None),
            P(),
            P("tp"),
            P(),
            P("tp", KV),
            P(KV),
            P(KV, "tp"),
            P(KV, "tp"),
            P("tp", KV),
        ),
        out_specs=P(None, KV),
        check_vma=False,
    )
```

```python
import jax
import jax.numpy as jnp
from jax import lax
from jax.experimental import pallas as pl
from jax.experimental.pallas import tpu as pltpu
from jax.sharding import Mesh
from jax.sharding import PartitionSpec as P

KV = ("z", "y")
EPS = 1e-06
FLOOR_SCORE = -1e30
BF = jnp.bfloat16
F32 = jnp.float32
VMEM = pl.BlockSpec(memory_space=pltpu.VMEM)
HBM = pl.BlockSpec(memory_space=pltpu.HBM)
INTERPRET = False


def run(kernel, outs, args, specs=None, scratch=(), grant=4):
    single = not isinstance(outs, (list, tuple))
    specs = specs or [VMEM] * len(args)
    if not INTERPRET:
        args = [
            pltpu.with_memory_space_constraint(a, s.memory_space) for a, s in zip(args, specs)
        ]
    return pl.pallas_call(
        kernel,
        out_shape=outs,
        in_specs=specs,
        out_specs=VMEM if single else [VMEM] * len(outs),
        scratch_shapes=scratch,
        compiler_params=pltpu.CompilerParams(vmem_limit_bytes=grant << 20),
        cost_estimate=pl.CostEstimate(flops=1000000000, bytes_accessed=40000000, transcendentals=0),
        interpret=INTERPRET,
    )(*args)


def shape(*dims, kind=BF):
    return jax.ShapeDtypeStruct(dims, kind) if INTERPRET else pltpu.VMEM(dims, kind)


def exchange(array, axis):
    return lax.all_to_all(array, axis, 0, 0, tiled=True)


def dot(left, right):
    return jnp.dot(left, right, preferred_element_type=F32)


def dot_t(left, right):
    return lax.dot_general(left, right, (((1,), (1,)), ((), ())), preferred_element_type=F32)


def rounded(array):
    return array.astype(BF).astype(F32)


def summed(ref):
    total = ref[0].astype(F32)
    for i in range(1, ref.shape[0]):
        total = total + ref[i].astype(F32)
    return total


def folded(term):
    return jnp.concatenate([term[0:8], term[8:16]], axis=1).astype(BF)


def unfolded(term):
    return jnp.concatenate([term[:, 0:64], term[:, 64:128]], axis=0)


def iota(shape_, dim):
    return lax.broadcasted_iota(jnp.int32, shape_, dim)


def as_row(column):
    here = iota((16, 128), 0) == iota((16, 128), 1)
    return jnp.sum(jnp.where(here, column, 0.0), axis=0, keepdims=True)


def as_column(row):
    here = iota((16, 128), 0) == iota((16, 128), 1)
    return jnp.sum(jnp.where(here, row, 0.0), axis=1, keepdims=True)


def project(
    tokens, gain, w_query, w_key, w_value, lengths, weight,
    out, limit, owner, picked, share,
    tokens_in, gain_in, query_in, key_in, value_in, lengths_in, weight_in, sems,
):
    pairs = (
        (tokens, tokens_in),
        (gain, gain_in),
        (w_query, query_in),
        (w_key, key_in),
        (w_value, value_in),
        (lengths, lengths_in),
        (weight, weight_in),
    )
    copies = [pltpu.make_async_copy(a, b, sems.at[i]) for i, (a, b) in enumerate(pairs)]
    for copy in copies:
        copy.start()
    z, y = lax.axis_index("z"), lax.axis_index("y")
    half, head = y // 4, y % 4
    start = (z * 8 + y) * 128
    mine = half * 8 + z
    row_head = iota((8, 128), 0) >> 1
    same_head = (iota((8, 128), 1) & 3) == row_head
    for b in range(16):
        own_row = jnp.logical_and(mine == b, row_head == head)
        owner[8 * b : 8 * b + 8, :] = jnp.where(own_row, 1, 0)
    picked[...] = jnp.where(iota((16, 128), 0) == mine, 1.0, 0.0)
    for copy in copies[:3]:
        copy.wait()
    x = tokens_in[...].astype(F32)
    scaled = (x * gain_in[...]).astype(BF)
    query = dot(scaled, query_in[...]).astype(BF)
    copies[3].wait()
    key = dot(scaled, key_in[...])
    copies[4].wait()
    value = dot(scaled, value_in[...])
    squares = as_row(jnp.sum(x * x, axis=1, keepdims=True))
    squares = jnp.broadcast_to(squares, (8, 128)).astype(BF)
    for i in range(8):
        rows = slice(8 * (i // 4), 8 * (i // 4) + 8)
        lanes = slice(128 * (i % 4), 128 * (i % 4) + 128)
        for h in range(4):
            out[i, 16 * h : 16 * h + 16, :] = query[:, 128 * h : 128 * h + 128]
        out[i, 64:80, :] = jnp.concatenate([key[rows, lanes], value[rows, lanes]], axis=0).astype(BF)
        out[i, 80:88, :] = squares
    for copy in copies[5:]:
        copy.wait()
    for b in range(16):
        limit[8 * b : 8 * b + 8, :] = jnp.where(same_head, lengths_in[b] - start, 0)
    lane_head = (iota((8, 128), 1) >> 1) & 3
    low = jnp.where(lane_head == 0, weight_in[0], weight_in[1])
    high = jnp.where(lane_head == 2, weight_in[2], weight_in[3])
    share[...] = jnp.where(lane_head < 2, low, high)


def relay(got, out):
    total = summed(got).astype(BF)
    for i in range(8):
        out[i] = total


def relay_query(got, out):
    total = summed(got)
    query = total[0:64].astype(BF)
    row = iota((8, 128), 0)
    for i in range(8):
        out[i, 0:64, :] = query
        key = total[64 + i : 65 + i]
        value = total[72 + i : 73 + i]
        last = jnp.where(row == 0, key, jnp.where(row == 1, value, total[80:81]))
        out[i, 64:72, :] = last.astype(BF)


def attend(got, keys, values, limit, owner, picked, out, rows_q, scores, acc):
    total = summed(got)
    inverse = lax.rsqrt(as_column(total[66:67]) / 4096 + EPS)
    first = iota((16, 128), 1) < 64
    for h in range(4):
        query = rounded(inverse * total[16 * h : 16 * h + 16])
        rows_q[pl.ds(2 * h, 16, stride=8), :] = jnp.where(first, query, 0.0)
        rows_q[pl.ds(2 * h + 1, 16, stride=8), :] = jnp.where(first, 0.0, query)
    for b in range(16):
        at = slice(8 * b, 8 * b + 8)
        scores[at, :] = dot_t(rows_q[at, :].astype(BF), keys[b])
    scale = jnp.sum(inverse * picked[...], axis=0, keepdims=True)
    key_new = rounded(scale * total[64:65])
    value_new = rounded(scale * total[65:66])
    owned = owner[...] > 0
    own = jnp.sum(rows_q[...] * key_new, axis=1, keepdims=True) * 0.125
    own = jnp.where(owned, own, FLOOR_SCORE)
    lane = iota((128, 128), 1)
    tiles, seen = [], []
    peak = own
    for t in range(4):
        visible = (lane + 128 * t) >> 2 < limit[...]
        tile = jnp.where(visible, scores[:, 128 * t : 128 * t + 128] * 0.125, FLOOR_SCORE)
        tiles.append(tile)
        seen.append(visible)
        peak = jnp.maximum(peak, tile)
    peak = jnp.max(peak, axis=1, keepdims=True)
    peak_hi = rounded(peak)
    peak_lo = rounded(peak - peak_hi)
    base = peak_hi + peak_lo
    weights = [jnp.where(v, jnp.exp(t - base), 0.0) for t, v in zip(tiles, seen)]
    own_weight = jnp.where(owned, jnp.exp(own - base), 0.0)
    totals = jnp.sum(weights[0] + weights[1] + weights[2] + weights[3], axis=1, keepdims=True)
    totals = totals + own_weight
    weights = jnp.concatenate(weights, axis=1).astype(BF)
    for b in range(16):
        at = slice(8 * b, 8 * b + 8)
        acc[at, :] = dot(weights[at, :], values[b])
    body = (acc[...] + rounded(own_weight) * value_new).T.astype(BF)
    totals_hi = rounded(totals)
    stat = jnp.where(
        lane == 0,
        peak_hi,
        jnp.where(lane == 1, peak_lo, jnp.where(lane == 2, totals_hi, totals - totals_hi)),
    )
    tail = stat.T[0:8].astype(BF)
    for i in range(8):
        out[i, 0:128, :] = body
        out[i, 128:136, :] = tail


def merged(got):
    tails = [got[i, 128:136, :].astype(F32) for i in range(8)]
    peaks = [t[0:1] + t[1:2] for t in tails]
    peak = peaks[0]
    for p in peaks[1:]:
        peak = jnp.maximum(peak, p)
    totals = jnp.zeros_like(peak)
    values = jnp.zeros((128, 128), F32)
    for i in range(8):
        scale = jnp.exp(peaks[i] - peak)
        totals = totals + scale * (tails[i][2:3] + tails[i][3:4])
        values = values + scale * got[i, 0:128, :].astype(F32)
    return peak, totals, values


def merge(got, out):
    peak, totals, values = merged(got)
    peak_hi, totals_hi = rounded(peak), rounded(totals)
    row = iota((8, 128), 0)
    tail = jnp.where(
        row == 0,
        peak_hi,
        jnp.where(row == 1, peak - peak_hi, jnp.where(row == 2, totals_hi, totals - totals_hi)),
    ).astype(BF)
    body = values.astype(BF)
    for i in range(8):
        out[i, 0:128, :] = body
        out[i, 128:136, :] = tail


def mix(got, share, head_gain, w_out, out, rows):
    _, totals, values = merged(got)
    ratio = values / totals
    mixture = ratio - share[0:1] * pltpu.roll(ratio, 127, 1)
    scale = lax.rsqrt(jnp.mean(mixture * mixture, axis=0, keepdims=True) + EPS)
    rows[...] = (mixture * scale).T * head_gain[...]
    attended = jnp.concatenate(
        [rows[pl.ds(2 * h, 16, stride=8), :] for h in range(4)], axis=1
    ).astype(BF)
    term = folded(dot_t(attended, w_out[...]))
    for i in range(8):
        out[i] = term


def widen(got, tokens, gain, w_gate, w_up, out, residual_out, rows):
    residual = (tokens[...].astype(F32) + unfolded(summed(got))).astype(BF)
    residual_out[...] = residual
    x = residual.astype(F32)
    scaled = (x * gain[...]).astype(BF)
    squares = jnp.broadcast_to(jnp.sum(x * x, axis=1, keepdims=True), (16, 128))
    for first, product in ((0, dot(scaled, w_gate[...])), (24, dot(scaled, w_up[...]))):
        for t in range(12):
            tile = product[:, 128 * t : 128 * t + 128] if t < 11 else squares
            rows[pl.ds(first + 2 * t, 8, stride=48), :] = tile[0:8]
            rows[pl.ds(first + 2 * t + 1, 8, stride=48), :] = tile[8:16]
    out[...] = rows[...].astype(BF)


def activate(got, out):
    total = summed(got)
    squares = jnp.where((iota((24, 128), 0) & 1) == 0, total[22:23], total[23:24])
    inverse = lax.rsqrt(squares / 4096 + EPS)
    gate = inverse * total[0:24]
    up = inverse * total[24:48]
    hidden = (gate / (1.0 + jnp.exp(-gate)) * up).astype(BF)
    for i in range(8):
        out[i] = hidden


def narrow(got, w_down, out, rows):
    rows[...] = got[...].astype(F32)
    halves = [
        jnp.concatenate([rows[pl.ds(2 * t + i, 8, stride=24), :] for t in range(11)], axis=1)
        for i in range(2)
    ]
    hidden = jnp.concatenate(halves, axis=0).astype(BF)
    term = folded(dot_t(hidden, w_down[...]))
    for i in range(8):
        out[i] = term


def finish(got, residual, out):
    out[...] = (residual[...].astype(F32) + unfolded(summed(got))).astype(BF)


def local(
    tokens,
    attn_gain,
    w_query,
    w_key,
    w_value,
    key_cache,
    value_cache,
    lengths,
    mix_weight,
    head_gain,
    w_out,
    mixer_gain,
    w_gate,
    w_up,
    w_down,
):
    tile = pltpu.VMEM((128, 128), F32)
    sent, limit, owner, picked, share = run(
        project,
        (
            shape(8, 88, 128),
            shape(128, 128, kind=jnp.int32),
            shape(128, 128, kind=jnp.int32),
            shape(16, 128, kind=F32),
            shape(8, 128, kind=F32),
        ),
        (
            tokens,
            attn_gain[None],
            w_query,
            w_key,
            w_value,
            lengths,
            mix_weight,
        ),
        specs=[HBM] * 7,
        scratch=[
            pltpu.VMEM((16, 64), BF),
            pltpu.VMEM((1, 64), F32),
            pltpu.VMEM((64, 512), BF),
            pltpu.VMEM((64, 512), BF),
            pltpu.VMEM((64, 512), BF),
            pltpu.SMEM((16,), jnp.int32),
            pltpu.SMEM((4,), F32),
            pltpu.SemaphoreType.DMA((7,)),
        ],
    )
    sent = run(relay_query, shape(8, 72, 128), (exchange(sent, "y"),))
    sent = run(
        attend,
        shape(8, 136, 128),
        (
            exchange(sent, "z"),
            key_cache.reshape(16, 512, 128),
            value_cache.reshape(16, 512, 128),
            limit,
            owner,
            picked,
        ),
        scratch=[tile, pltpu.VMEM((128, 512), F32), tile],
    )
    sent = run(merge, shape(8, 136, 128), (exchange(sent, "z"),))
    sent = run(
        mix,
        shape(8, 8, 128),
        (exchange(sent, "y"), share, head_gain[None], w_out.T),
        scratch=[tile],
    )
    sent, residual = run(
        widen,
        (shape(384, 128), shape(16, 64)),
        (exchange(sent, "tp"), tokens, mixer_gain[None], w_gate, w_up),
        scratch=[pltpu.VMEM((384, 128), F32)],
    )
    sent = run(relay, shape(8, 48, 128), (exchange(sent.reshape(8, 48, 128), "y"),))
    sent = run(activate, shape(8, 24, 128), (exchange(sent, "z"),))
    sent = run(
        narrow,
        shape(8, 8, 128),
        (exchange(sent, "y").reshape(192, 128), w_down.T),
        scratch=[pltpu.VMEM((192, 128), F32)],
    )
    return run(finish, jax.ShapeDtypeStruct((16, 64), BF), (exchange(sent, "tp"), residual))


def solution(mesh):
    finer = Mesh(mesh.devices.reshape(8, 8, mesh.shape["tp"]), ("z", "y", "tp"))
    return jax.shard_map(
        local,
        mesh=finer,
        in_specs=(
            P(None, KV),
            P(KV),
            P(KV, "tp"),
            P(KV, "tp"),
            P(KV, "tp"),
            P(None, KV, "tp", None),
            P(None, KV, "tp", None),
            P(),
            P("tp"),
            P(),
            P("tp", KV),
            P(KV),
            P(KV, "tp"),
            P(KV, "tp"),
            P("tp", KV),
        ),
        out_specs=P(None, KV),
        check_vma=False,
    )
```

```python
import jax
import jax.numpy as jnp
from jax import lax
from jax.experimental import pallas as pl
from jax.experimental.pallas import tpu as pltpu
from jax.sharding import Mesh
from jax.sharding import PartitionSpec as P

KV = ("z", "y")
ALL = ("z", "y", "tp")


def lines(along_y_on):
    found = []
    for t in range(8):
        for fixed in range(8):
            if t % 2 == along_y_on:
                found.append([(fixed * 8 + y) * 8 + t for y in range(8)])
            else:
                found.append([(z * 8 + fixed) * 8 + t for z in range(8)])
    return found


U, W = lines(0), lines(1)
EPS = 1e-06
FLOOR_SCORE = -1e30
BF = jnp.bfloat16
F32 = jnp.float32
VMEM = pl.BlockSpec(memory_space=pltpu.VMEM)
HBM = pl.BlockSpec(memory_space=pltpu.HBM)
INTERPRET = False


def run(kernel, outs, args, specs=None, scratch=(), grant=4):
    single = not isinstance(outs, (list, tuple))
    specs = specs or [VMEM] * len(args)
    if not INTERPRET:
        args = [
            pltpu.with_memory_space_constraint(a, s.memory_space) for a, s in zip(args, specs)
        ]
    return pl.pallas_call(
        kernel,
        out_shape=outs,
        in_specs=specs,
        out_specs=VMEM if single else [VMEM] * len(outs),
        scratch_shapes=scratch,
        compiler_params=pltpu.CompilerParams(vmem_limit_bytes=grant << 20),
        cost_estimate=pl.CostEstimate(flops=1000000000, bytes_accessed=40000000, transcendentals=0),
        interpret=INTERPRET,
    )(*args)


def shape(*dims, kind=BF):
    return jax.ShapeDtypeStruct(dims, kind) if INTERPRET else pltpu.VMEM(dims, kind)


def exchange(array, axis, groups=None):
    return lax.all_to_all(array, axis, 0, 0, axis_index_groups=groups, tiled=True)


def dot(left, right):
    return jnp.dot(left, right, preferred_element_type=F32)


def dot_t(left, right):
    return lax.dot_general(left, right, (((1,), (1,)), ((), ())), preferred_element_type=F32)


def rounded(array):
    return array.astype(BF).astype(F32)


def summed(ref):
    total = ref[0].astype(F32)
    for i in range(1, ref.shape[0]):
        total = total + ref[i].astype(F32)
    return total


def folded(term):
    return jnp.concatenate([term[0:8], term[8:16]], axis=1).astype(BF)


def unfolded(term):
    return jnp.concatenate([term[:, 0:64], term[:, 64:128]], axis=0)


def iota(shape_, dim):
    return lax.broadcasted_iota(jnp.int32, shape_, dim)


def as_row(column):
    here = iota((16, 128), 0) == iota((16, 128), 1)
    return jnp.sum(jnp.where(here, column, 0.0), axis=0, keepdims=True)


def as_column(row):
    here = iota((16, 128), 0) == iota((16, 128), 1)
    return jnp.sum(jnp.where(here, row, 0.0), axis=1, keepdims=True)


def project(
    tokens, gain, w_query, w_key, w_value, lengths, weight,
    out, limit, owner, picked, share,
    tokens_in, gain_in, query_in, key_in, value_in, lengths_in, weight_in, sems,
):
    pairs = (
        (tokens, tokens_in),
        (gain, gain_in),
        (w_query, query_in),
        (w_key, key_in),
        (w_value, value_in),
        (lengths, lengths_in),
        (weight, weight_in),
    )
    copies = [pltpu.make_async_copy(a, b, sems.at[i]) for i, (a, b) in enumerate(pairs)]
    for copy in copies:
        copy.start()
    z, y, even = lax.axis_index("z"), lax.axis_index("y"), lax.axis_index("tp") % 2 == 0
    u, w = jnp.where(even, y, z), jnp.where(even, z, y)
    half, head = u // 4, u % 4
    start = (z * 8 + y) * 128
    mine = half * 8 + w
    row_head = iota((8, 128), 0) >> 1
    same_head = (iota((8, 128), 1) & 3) == row_head
    for b in range(16):
        own_row = jnp.logical_and(mine == b, row_head == head)
        owner[8 * b : 8 * b + 8, :] = jnp.where(own_row, 1, 0)
    picked[...] = jnp.where(iota((16, 128), 0) == mine, 1.0, 0.0)
    for copy in copies[:3]:
        copy.wait()
    x = tokens_in[...].astype(F32)
    scaled = (x * gain_in[...]).astype(BF)
    query = dot(scaled, query_in[...]).astype(BF)
    copies[3].wait()
    key = dot(scaled, key_in[...])
    copies[4].wait()
    value = dot(scaled, value_in[...])
    squares = as_row(jnp.sum(x * x, axis=1, keepdims=True))
    squares = jnp.broadcast_to(squares, (8, 128)).astype(BF)
    for i in range(8):
        rows = slice(8 * (i // 4), 8 * (i // 4) + 8)
        lanes = slice(128 * (i % 4), 128 * (i % 4) + 128)
        for h in range(4):
            out[i, 16 * h : 16 * h + 16, :] = query[:, 128 * h : 128 * h + 128]
        out[i, 64:80, :] = jnp.concatenate([key[rows, lanes], value[rows, lanes]], axis=0).astype(BF)
        out[i, 80:88, :] = squares
    for copy in copies[5:]:
        copy.wait()
    for b in range(16):
        limit[8 * b : 8 * b + 8, :] = jnp.where(same_head, lengths_in[b] - start, 0)
    lane_head = (iota((8, 128), 1) >> 1) & 3
    low = jnp.where(lane_head == 0, weight_in[0], weight_in[1])
    high = jnp.where(lane_head == 2, weight_in[2], weight_in[3])
    share[...] = jnp.where(lane_head < 2, low, high)


def relay(got, out):
    total = summed(got).astype(BF)
    for i in range(8):
        out[i] = total


def relay_query(got, out):
    total = summed(got)
    query = total[0:64].astype(BF)
    row = iota((8, 128), 0)
    for i in range(8):
        out[i, 0:64, :] = query
        key = total[64 + i : 65 + i]
        value = total[72 + i : 73 + i]
        last = jnp.where(row == 0, key, jnp.where(row == 1, value, total[80:81]))
        out[i, 64:72, :] = last.astype(BF)


def attend(got, keys, values, limit, owner, picked, out, rows_q, scores, acc):
    total = summed(got)
    inverse = lax.rsqrt(as_column(total[66:67]) / 4096 + EPS)
    first = iota((16, 128), 1) < 64
    for h in range(4):
        query = rounded(inverse * total[16 * h : 16 * h + 16])
        rows_q[pl.ds(2 * h, 16, stride=8), :] = jnp.where(first, query, 0.0)
        rows_q[pl.ds(2 * h + 1, 16, stride=8), :] = jnp.where(first, 0.0, query)
    for b in range(16):
        at = slice(8 * b, 8 * b + 8)
        scores[at, :] = dot_t(rows_q[at, :].astype(BF), keys[b])
    scale = jnp.sum(inverse * picked[...], axis=0, keepdims=True)
    key_new = rounded(scale * total[64:65])
    value_new = rounded(scale * total[65:66])
    owned = owner[...] > 0
    own = jnp.sum(rows_q[...] * key_new, axis=1, keepdims=True) * 0.125
    own = jnp.where(owned, own, FLOOR_SCORE)
    lane = iota((128, 128), 1)
    tiles, seen = [], []
    peak = own
    for t in range(4):
        visible = (lane + 128 * t) >> 2 < limit[...]
        tile = jnp.where(visible, scores[:, 128 * t : 128 * t + 128] * 0.125, FLOOR_SCORE)
        tiles.append(tile)
        seen.append(visible)
        peak = jnp.maximum(peak, tile)
    peak = jnp.max(peak, axis=1, keepdims=True)
    peak_hi = rounded(peak)
    peak_lo = rounded(peak - peak_hi)
    base = peak_hi + peak_lo
    weights = [jnp.where(v, jnp.exp(t - base), 0.0) for t, v in zip(tiles, seen)]
    own_weight = jnp.where(owned, jnp.exp(own - base), 0.0)
    totals = jnp.sum(weights[0] + weights[1] + weights[2] + weights[3], axis=1, keepdims=True)
    totals = totals + own_weight
    weights = jnp.concatenate(weights, axis=1).astype(BF)
    for b in range(16):
        at = slice(8 * b, 8 * b + 8)
        acc[at, :] = dot(weights[at, :], values[b])
    body = (acc[...] + rounded(own_weight) * value_new).T.astype(BF)
    totals_hi = rounded(totals)
    stat = jnp.where(
        lane == 0,
        peak_hi,
        jnp.where(lane == 1, peak_lo, jnp.where(lane == 2, totals_hi, totals - totals_hi)),
    )
    tail = stat.T[0:8].astype(BF)
    for i in range(8):
        out[i, 0:128, :] = body
        out[i, 128:136, :] = tail


def merged(got):
    tails = [got[i, 128:136, :].astype(F32) for i in range(8)]
    peaks = [t[0:1] + t[1:2] for t in tails]
    peak = peaks[0]
    for p in peaks[1:]:
        peak = jnp.maximum(peak, p)
    totals = jnp.zeros_like(peak)
    values = jnp.zeros((128, 128), F32)
    for i in range(8):
        scale = jnp.exp(peaks[i] - peak)
        totals = totals + scale * (tails[i][2:3] + tails[i][3:4])
        values = values + scale * got[i, 0:128, :].astype(F32)
    return peak, totals, values


def merge(got, out):
    peak, totals, values = merged(got)
    peak_hi, totals_hi = rounded(peak), rounded(totals)
    row = iota((8, 128), 0)
    tail = jnp.where(
        row == 0,
        peak_hi,
        jnp.where(row == 1, peak - peak_hi, jnp.where(row == 2, totals_hi, totals - totals_hi)),
    ).astype(BF)
    body = values.astype(BF)
    for i in range(8):
        out[i, 0:128, :] = body
        out[i, 128:136, :] = tail


def mix(got, share, head_gain, w_out, out, rows):
    _, totals, values = merged(got)
    ratio = values / totals
    mixture = ratio - share[0:1] * pltpu.roll(ratio, 127, 1)
    scale = lax.rsqrt(jnp.mean(mixture * mixture, axis=0, keepdims=True) + EPS)
    rows[...] = (mixture * scale).T * head_gain[...]
    attended = jnp.concatenate(
        [rows[pl.ds(2 * h, 16, stride=8), :] for h in range(4)], axis=1
    ).astype(BF)
    term = folded(dot_t(attended, w_out[...]))
    for i in range(8):
        out[i] = term


def widen(got, tokens, gain, w_gate, w_up, out, residual_out, rows):
    residual = (tokens[...].astype(F32) + unfolded(summed(got))).astype(BF)
    residual_out[...] = residual
    x = residual.astype(F32)
    scaled = (x * gain[...]).astype(BF)
    squares = jnp.broadcast_to(jnp.sum(x * x, axis=1, keepdims=True), (16, 128))
    for first, product in ((0, dot(scaled, w_gate[...])), (24, dot(scaled, w_up[...]))):
        for t in range(12):
            tile = product[:, 128 * t : 128 * t + 128] if t < 11 else squares
            rows[pl.ds(first + 2 * t, 8, stride=48), :] = tile[0:8]
            rows[pl.ds(first + 2 * t + 1, 8, stride=48), :] = tile[8:16]
    out[...] = rows[...].astype(BF)


def activate(got, out):
    total = summed(got)
    squares = jnp.where((iota((24, 128), 0) & 1) == 0, total[22:23], total[23:24])
    inverse = lax.rsqrt(squares / 4096 + EPS)
    gate = inverse * total[0:24]
    up = inverse * total[24:48]
    hidden = (gate / (1.0 + jnp.exp(-gate)) * up).astype(BF)
    for i in range(8):
        out[i] = hidden


def narrow(got, w_down, out, rows):
    rows[...] = got[...].astype(F32)
    halves = [
        jnp.concatenate([rows[pl.ds(2 * t + i, 8, stride=24), :] for t in range(11)], axis=1)
        for i in range(2)
    ]
    hidden = jnp.concatenate(halves, axis=0).astype(BF)
    term = folded(dot_t(hidden, w_down[...]))
    for i in range(8):
        out[i] = term


def finish(got, residual, out):
    out[...] = (residual[...].astype(F32) + unfolded(summed(got))).astype(BF)


def local(
    tokens,
    attn_gain,
    w_query,
    w_key,
    w_value,
    key_cache,
    value_cache,
    lengths,
    mix_weight,
    head_gain,
    w_out,
    mixer_gain,
    w_gate,
    w_up,
    w_down,
):
    tile = pltpu.VMEM((128, 128), F32)
    sent, limit, owner, picked, share = run(
        project,
        (
            shape(8, 88, 128),
            shape(128, 128, kind=jnp.int32),
            shape(128, 128, kind=jnp.int32),
            shape(16, 128, kind=F32),
            shape(8, 128, kind=F32),
        ),
        (
            tokens,
            attn_gain[None],
            w_query,
            w_key,
            w_value,
            lengths,
            mix_weight,
        ),
        specs=[HBM] * 7,
        scratch=[
            pltpu.VMEM((16, 64), BF),
            pltpu.VMEM((1, 64), F32),
            pltpu.VMEM((64, 512), BF),
            pltpu.VMEM((64, 512), BF),
            pltpu.VMEM((64, 512), BF),
            pltpu.SMEM((16,), jnp.int32),
            pltpu.SMEM((4,), F32),
            pltpu.SemaphoreType.DMA((7,)),
        ],
    )
    sent = run(relay_query, shape(8, 72, 128), (exchange(sent, ALL, U),))
    sent = run(
        attend,
        shape(8, 136, 128),
        (
            exchange(sent, ALL, W),
            key_cache.reshape(16, 512, 128),
            value_cache.reshape(16, 512, 128),
            limit,
            owner,
            picked,
        ),
        scratch=[tile, pltpu.VMEM((128, 512), F32), tile],
    )
    sent = run(merge, shape(8, 136, 128), (exchange(sent, ALL, W),))
    sent = run(
        mix,
        shape(8, 8, 128),
        (exchange(sent, ALL, U), share, head_gain[None], w_out.T),
        scratch=[tile],
    )
    sent, residual = run(
        widen,
        (shape(384, 128), shape(16, 64)),
        (exchange(sent, "tp"), tokens, mixer_gain[None], w_gate, w_up),
        scratch=[pltpu.VMEM((384, 128), F32)],
    )
    sent = run(relay, shape(8, 48, 128), (exchange(sent.reshape(8, 48, 128), ALL, U),))
    sent = run(activate, shape(8, 24, 128), (exchange(sent, ALL, W),))
    sent = run(
        narrow,
        shape(8, 8, 128),
        (exchange(sent, ALL, U).reshape(192, 128), w_down.T),
        scratch=[pltpu.VMEM((192, 128), F32)],
    )
    return run(finish, jax.ShapeDtypeStruct((16, 64), BF), (exchange(sent, "tp"), residual))


def solution(mesh):
    finer = Mesh(mesh.devices.reshape(8, 8, mesh.shape["tp"]), ("z", "y", "tp"))
    return jax.shard_map(
        local,
        mesh=finer,
        in_specs=(
            P(None, KV),
            P(KV),
            P(KV, "tp"),
            P(KV, "tp"),
            P(KV, "tp"),
            P(None, KV, "tp", None),
            P(None, KV, "tp", None),
            P(),
            P("tp"),
            P(),
            P("tp", KV),
            P(KV),
            P(KV, "tp"),
            P(KV, "tp"),
            P("tp", KV),
        ),
        out_specs=P(None, KV),
        check_vma=False,
    )
```

```python
import jax
import jax.numpy as jnp
from jax import lax
from jax.experimental import pallas as pl
from jax.experimental.pallas import tpu as pltpu
from jax.sharding import Mesh
from jax.sharding import PartitionSpec as P

KV = ("z", "y")
ALL = ("z", "y", "tp")


ORDER = [0, 4, 1, 5, 2, 6, 3, 7]


def spot(coordinate):
    return 2 * (coordinate % 4) + coordinate // 4


def lines(along_y_on):
    found = []
    for t in range(8):
        for fixed in range(8):
            if t % 2 == along_y_on:
                found.append([(fixed * 8 + y) * 8 + t for y in ORDER])
            else:
                found.append([(z * 8 + fixed) * 8 + t for z in ORDER])
    return found


U, W = lines(0), lines(1)
EPS = 1e-06
FLOOR_SCORE = -1e30
BF = jnp.bfloat16
F32 = jnp.float32
VMEM = pl.BlockSpec(memory_space=pltpu.VMEM)
HBM = pl.BlockSpec(memory_space=pltpu.HBM)
INTERPRET = False


def run(kernel, outs, args, specs=None, scratch=(), grant=4):
    single = not isinstance(outs, (list, tuple))
    specs = specs or [VMEM] * len(args)
    if not INTERPRET:
        args = [
            pltpu.with_memory_space_constraint(a, s.memory_space) for a, s in zip(args, specs)
        ]
    return pl.pallas_call(
        kernel,
        out_shape=outs,
        in_specs=specs,
        out_specs=VMEM if single else [VMEM] * len(outs),
        scratch_shapes=scratch,
        compiler_params=pltpu.CompilerParams(vmem_limit_bytes=grant << 20),
        cost_estimate=pl.CostEstimate(flops=1000000000, bytes_accessed=40000000, transcendentals=0),
        interpret=INTERPRET,
    )(*args)


def shape(*dims, kind=BF):
    return jax.ShapeDtypeStruct(dims, kind) if INTERPRET else pltpu.VMEM(dims, kind)


def exchange(array, axis, groups=None):
    return lax.all_to_all(array, axis, 0, 0, axis_index_groups=groups, tiled=True)


def dot(left, right):
    return jnp.dot(left, right, preferred_element_type=F32)


def dot_t(left, right):
    return lax.dot_general(left, right, (((1,), (1,)), ((), ())), preferred_element_type=F32)


def rounded(array):
    return array.astype(BF).astype(F32)


def summed(ref):
    total = ref[0].astype(F32)
    for i in range(1, ref.shape[0]):
        total = total + ref[i].astype(F32)
    return total


def folded(term):
    return jnp.concatenate([term[0:8], term[8:16]], axis=1).astype(BF)


def unfolded(term):
    return jnp.concatenate([term[:, 0:64], term[:, 64:128]], axis=0)


def iota(shape_, dim):
    return lax.broadcasted_iota(jnp.int32, shape_, dim)


def as_row(column):
    here = iota((16, 128), 0) == iota((16, 128), 1)
    return jnp.sum(jnp.where(here, column, 0.0), axis=0, keepdims=True)


def as_column(row):
    here = iota((16, 128), 0) == iota((16, 128), 1)
    return jnp.sum(jnp.where(here, row, 0.0), axis=1, keepdims=True)


def project(
    tokens, gain, w_query, w_key, w_value, lengths, weight,
    out, limit, owner, picked, share,
    tokens_in, gain_in, query_in, key_in, value_in, lengths_in, weight_in, sems,
):
    pairs = (
        (tokens, tokens_in),
        (gain, gain_in),
        (w_query, query_in),
        (w_key, key_in),
        (w_value, value_in),
        (lengths, lengths_in),
        (weight, weight_in),
    )
    copies = [pltpu.make_async_copy(a, b, sems.at[i]) for i, (a, b) in enumerate(pairs)]
    for copy in copies:
        copy.start()
    z, y, even = lax.axis_index("z"), lax.axis_index("y"), lax.axis_index("tp") % 2 == 0
    u, w = spot(jnp.where(even, y, z)), spot(jnp.where(even, z, y))
    half, head = u // 4, u % 4
    start = (z * 8 + y) * 128
    mine = half * 8 + w
    row_head = iota((8, 128), 0) >> 1
    same_head = (iota((8, 128), 1) & 3) == row_head
    for b in range(16):
        own_row = jnp.logical_and(mine == b, row_head == head)
        owner[8 * b : 8 * b + 8, :] = jnp.where(own_row, 1, 0)
    picked[...] = jnp.where(iota((16, 128), 0) == mine, 1.0, 0.0)
    for copy in copies[:3]:
        copy.wait()
    x = tokens_in[...].astype(F32)
    scaled = (x * gain_in[...]).astype(BF)
    query = dot(scaled, query_in[...]).astype(BF)
    copies[3].wait()
    key = dot(scaled, key_in[...])
    copies[4].wait()
    value = dot(scaled, value_in[...])
    squares = as_row(jnp.sum(x * x, axis=1, keepdims=True))
    squares = jnp.broadcast_to(squares, (8, 128)).astype(BF)
    for i in range(8):
        rows = slice(8 * (i // 4), 8 * (i // 4) + 8)
        lanes = slice(128 * (i % 4), 128 * (i % 4) + 128)
        for h in range(4):
            out[i, 16 * h : 16 * h + 16, :] = query[:, 128 * h : 128 * h + 128]
        out[i, 64:80, :] = jnp.concatenate([key[rows, lanes], value[rows, lanes]], axis=0).astype(BF)
        out[i, 80:88, :] = squares
    for copy in copies[5:]:
        copy.wait()
    for b in range(16):
        limit[8 * b : 8 * b + 8, :] = jnp.where(same_head, lengths_in[b] - start, 0)
    lane_head = (iota((8, 128), 1) >> 1) & 3
    low = jnp.where(lane_head == 0, weight_in[0], weight_in[1])
    high = jnp.where(lane_head == 2, weight_in[2], weight_in[3])
    share[...] = jnp.where(lane_head < 2, low, high)


def relay(got, out):
    total = summed(got).astype(BF)
    for i in range(8):
        out[i] = total


def relay_query(got, out):
    total = summed(got)
    query = total[0:64].astype(BF)
    row = iota((8, 128), 0)
    for i in range(8):
        out[i, 0:64, :] = query
        key = total[64 + i : 65 + i]
        value = total[72 + i : 73 + i]
        last = jnp.where(row == 0, key, jnp.where(row == 1, value, total[80:81]))
        out[i, 64:72, :] = last.astype(BF)


def attend(got, keys, values, limit, owner, picked, out, rows_q, scores, acc):
    total = summed(got)
    inverse = lax.rsqrt(as_column(total[66:67]) / 4096 + EPS)
    first = iota((16, 128), 1) < 64
    for h in range(4):
        query = rounded(inverse * total[16 * h : 16 * h + 16])
        rows_q[pl.ds(2 * h, 16, stride=8), :] = jnp.where(first, query, 0.0)
        rows_q[pl.ds(2 * h + 1, 16, stride=8), :] = jnp.where(first, 0.0, query)
    for b in range(16):
        at = slice(8 * b, 8 * b + 8)
        scores[at, :] = dot_t(rows_q[at, :].astype(BF), keys[b])
    scale = jnp.sum(inverse * picked[...], axis=0, keepdims=True)
    key_new = rounded(scale * total[64:65])
    value_new = rounded(scale * total[65:66])
    owned = owner[...] > 0
    own = jnp.sum(rows_q[...] * key_new, axis=1, keepdims=True) * 0.125
    own = jnp.where(owned, own, FLOOR_SCORE)
    lane = iota((128, 128), 1)
    tiles, seen = [], []
    peak = own
    for t in range(4):
        visible = (lane + 128 * t) >> 2 < limit[...]
        tile = jnp.where(visible, scores[:, 128 * t : 128 * t + 128] * 0.125, FLOOR_SCORE)
        tiles.append(tile)
        seen.append(visible)
        peak = jnp.maximum(peak, tile)
    peak = jnp.max(peak, axis=1, keepdims=True)
    peak_hi = rounded(peak)
    peak_lo = rounded(peak - peak_hi)
    base = peak_hi + peak_lo
    weights = [jnp.where(v, jnp.exp(t - base), 0.0) for t, v in zip(tiles, seen)]
    own_weight = jnp.where(owned, jnp.exp(own - base), 0.0)
    totals = jnp.sum(weights[0] + weights[1] + weights[2] + weights[3], axis=1, keepdims=True)
    totals = totals + own_weight
    weights = jnp.concatenate(weights, axis=1).astype(BF)
    for b in range(16):
        at = slice(8 * b, 8 * b + 8)
        acc[at, :] = dot(weights[at, :], values[b])
    body = (acc[...] + rounded(own_weight) * value_new).T.astype(BF)
    totals_hi = rounded(totals)
    stat = jnp.where(
        lane == 0,
        peak_hi,
        jnp.where(lane == 1, peak_lo, jnp.where(lane == 2, totals_hi, totals - totals_hi)),
    )
    tail = stat.T[0:8].astype(BF)
    for i in range(8):
        out[i, 0:128, :] = body
        out[i, 128:136, :] = tail


def merged(got):
    tails = [got[i, 128:136, :].astype(F32) for i in range(8)]
    peaks = [t[0:1] + t[1:2] for t in tails]
    peak = peaks[0]
    for p in peaks[1:]:
        peak = jnp.maximum(peak, p)
    totals = jnp.zeros_like(peak)
    values = jnp.zeros((128, 128), F32)
    for i in range(8):
        scale = jnp.exp(peaks[i] - peak)
        totals = totals + scale * (tails[i][2:3] + tails[i][3:4])
        values = values + scale * got[i, 0:128, :].astype(F32)
    return peak, totals, values


def merge(got, out):
    peak, totals, values = merged(got)
    peak_hi, totals_hi = rounded(peak), rounded(totals)
    row = iota((8, 128), 0)
    tail = jnp.where(
        row == 0,
        peak_hi,
        jnp.where(row == 1, peak - peak_hi, jnp.where(row == 2, totals_hi, totals - totals_hi)),
    ).astype(BF)
    body = values.astype(BF)
    for i in range(8):
        out[i, 0:128, :] = body
        out[i, 128:136, :] = tail


def mix(got, share, head_gain, w_out, out, rows):
    _, totals, values = merged(got)
    ratio = values / totals
    mixture = ratio - share[0:1] * pltpu.roll(ratio, 127, 1)
    scale = lax.rsqrt(jnp.mean(mixture * mixture, axis=0, keepdims=True) + EPS)
    rows[...] = (mixture * scale).T * head_gain[...]
    attended = jnp.concatenate(
        [rows[pl.ds(2 * h, 16, stride=8), :] for h in range(4)], axis=1
    ).astype(BF)
    term = folded(dot_t(attended, w_out[...]))
    for i in range(8):
        out[i] = term


def widen(got, tokens, gain, w_gate, w_up, out, residual_out, rows):
    residual = (tokens[...].astype(F32) + unfolded(summed(got))).astype(BF)
    residual_out[...] = residual
    x = residual.astype(F32)
    scaled = (x * gain[...]).astype(BF)
    squares = jnp.broadcast_to(jnp.sum(x * x, axis=1, keepdims=True), (16, 128))
    for first, product in ((0, dot(scaled, w_gate[...])), (24, dot(scaled, w_up[...]))):
        for t in range(12):
            tile = product[:, 128 * t : 128 * t + 128] if t < 11 else squares
            rows[pl.ds(first + 2 * t, 8, stride=48), :] = tile[0:8]
            rows[pl.ds(first + 2 * t + 1, 8, stride=48), :] = tile[8:16]
    out[...] = rows[...].astype(BF)


def activate(got, out):
    total = summed(got)
    squares = jnp.where((iota((24, 128), 0) & 1) == 0, total[22:23], total[23:24])
    inverse = lax.rsqrt(squares / 4096 + EPS)
    gate = inverse * total[0:24]
    up = inverse * total[24:48]
    hidden = (gate / (1.0 + jnp.exp(-gate)) * up).astype(BF)
    for i in range(8):
        out[i] = hidden


def narrow(got, w_down, out, rows):
    rows[...] = got[...].astype(F32)
    halves = [
        jnp.concatenate([rows[pl.ds(2 * t + i, 8, stride=24), :] for t in range(11)], axis=1)
        for i in range(2)
    ]
    hidden = jnp.concatenate(halves, axis=0).astype(BF)
    term = folded(dot_t(hidden, w_down[...]))
    for i in range(8):
        out[i] = term


def finish(got, residual, out):
    out[...] = (residual[...].astype(F32) + unfolded(summed(got))).astype(BF)


def local(
    tokens,
    attn_gain,
    w_query,
    w_key,
    w_value,
    key_cache,
    value_cache,
    lengths,
    mix_weight,
    head_gain,
    w_out,
    mixer_gain,
    w_gate,
    w_up,
    w_down,
):
    tile = pltpu.VMEM((128, 128), F32)
    sent, limit, owner, picked, share = run(
        project,
        (
            shape(8, 88, 128),
            shape(128, 128, kind=jnp.int32),
            shape(128, 128, kind=jnp.int32),
            shape(16, 128, kind=F32),
            shape(8, 128, kind=F32),
        ),
        (
            tokens,
            attn_gain[None],
            w_query,
            w_key,
            w_value,
            lengths,
            mix_weight,
        ),
        specs=[HBM] * 7,
        scratch=[
            pltpu.VMEM((16, 64), BF),
            pltpu.VMEM((1, 64), F32),
            pltpu.VMEM((64, 512), BF),
            pltpu.VMEM((64, 512), BF),
            pltpu.VMEM((64, 512), BF),
            pltpu.SMEM((16,), jnp.int32),
            pltpu.SMEM((4,), F32),
            pltpu.SemaphoreType.DMA((7,)),
        ],
    )
    sent = run(relay_query, shape(8, 72, 128), (exchange(sent, ALL, U),))
    sent = run(
        attend,
        shape(8, 136, 128),
        (
            exchange(sent, ALL, W),
            key_cache.reshape(16, 512, 128),
            value_cache.reshape(16, 512, 128),
            limit,
            owner,
            picked,
        ),
        scratch=[tile, pltpu.VMEM((128, 512), F32), tile],
    )
    sent = run(merge, shape(8, 136, 128), (exchange(sent, ALL, W),))
    sent = run(
        mix,
        shape(8, 8, 128),
        (exchange(sent, ALL, U), share, head_gain[None], w_out.T),
        scratch=[tile],
    )
    sent, residual = run(
        widen,
        (shape(384, 128), shape(16, 64)),
        (exchange(sent, "tp"), tokens, mixer_gain[None], w_gate, w_up),
        scratch=[pltpu.VMEM((384, 128), F32)],
    )
    sent = run(relay, shape(8, 48, 128), (exchange(sent.reshape(8, 48, 128), ALL, U),))
    sent = run(activate, shape(8, 24, 128), (exchange(sent, ALL, W),))
    sent = run(
        narrow,
        shape(8, 8, 128),
        (exchange(sent, ALL, U).reshape(192, 128), w_down.T),
        scratch=[pltpu.VMEM((192, 128), F32)],
    )
    return run(finish, jax.ShapeDtypeStruct((16, 64), BF), (exchange(sent, "tp"), residual))


def solution(mesh):
    finer = Mesh(mesh.devices.reshape(8, 8, mesh.shape["tp"]), ("z", "y", "tp"))
    return jax.shard_map(
        local,
        mesh=finer,
        in_specs=(
            P(None, KV),
            P(KV),
            P(KV, "tp"),
            P(KV, "tp"),
            P(KV, "tp"),
            P(None, KV, "tp", None),
            P(None, KV, "tp", None),
            P(),
            P("tp"),
            P(),
            P("tp", KV),
            P(KV),
            P(KV, "tp"),
            P(KV, "tp"),
            P("tp", KV),
        ),
        out_specs=P(None, KV),
        check_vma=False,
    )
```

```python
import jax
import jax.numpy as jnp
from jax import lax
from jax.experimental import pallas as pl
from jax.experimental.pallas import tpu as pltpu
from jax.sharding import Mesh
from jax.sharding import PartitionSpec as P

KV = ("z", "y")
ALL = ("z", "y", "tp")


ORDER = [0, 4, 1, 5, 2, 6, 3, 7]


def spot(coordinate):
    return 2 * (coordinate % 4) + coordinate // 4


def lines(along_y_on):
    found = []
    for t in range(8):
        for fixed in range(8):
            if t % 2 == along_y_on:
                found.append([(fixed * 8 + y) * 8 + t for y in ORDER])
            else:
                found.append([(z * 8 + fixed) * 8 + t for z in ORDER])
    return found


U, W = lines(0), lines(1)
EPS = 1e-06
FLOOR_SCORE = -1e30
BF = jnp.bfloat16
F32 = jnp.float32
VMEM = pl.BlockSpec(memory_space=pltpu.VMEM)
HBM = pl.BlockSpec(memory_space=pltpu.HBM)
INTERPRET = False


def run(kernel, outs, args, specs=None, scratch=(), grant=4, flags=None):
    single = not isinstance(outs, (list, tuple))
    specs = specs or [VMEM] * len(args)
    if not INTERPRET:
        args = [
            pltpu.with_memory_space_constraint(a, s.memory_space) for a, s in zip(args, specs)
        ]
    return pl.pallas_call(
        kernel,
        out_shape=outs,
        in_specs=specs,
        out_specs=VMEM if single else [VMEM] * len(outs),
        scratch_shapes=scratch,
        compiler_params=pltpu.CompilerParams(vmem_limit_bytes=grant << 20, flags=flags),
        cost_estimate=pl.CostEstimate(flops=1000000000, bytes_accessed=40000000, transcendentals=0),
        interpret=INTERPRET,
    )(*args)


def shape(*dims, kind=BF):
    return jax.ShapeDtypeStruct(dims, kind) if INTERPRET else pltpu.VMEM(dims, kind)


def exchange(array, axis, groups=None):
    return lax.all_to_all(array, axis, 0, 0, axis_index_groups=groups, tiled=True)


def dot(left, right):
    return jnp.dot(left, right, preferred_element_type=F32)


def dot_t(left, right):
    return lax.dot_general(left, right, (((1,), (1,)), ((), ())), preferred_element_type=F32)


def rounded(array):
    return array.astype(BF).astype(F32)


def summed(ref):
    total = ref[0].astype(F32)
    for i in range(1, ref.shape[0]):
        total = total + ref[i].astype(F32)
    return total


def folded(term):
    return jnp.concatenate([term[0:8], term[8:16]], axis=1).astype(BF)


def unfolded(term):
    return jnp.concatenate([term[:, 0:64], term[:, 64:128]], axis=0)


def iota(shape_, dim):
    return lax.broadcasted_iota(jnp.int32, shape_, dim)


def as_row(column):
    here = iota((16, 128), 0) == iota((16, 128), 1)
    return jnp.sum(jnp.where(here, column, 0.0), axis=0, keepdims=True)


def as_column(row):
    here = iota((16, 128), 0) == iota((16, 128), 1)
    return jnp.sum(jnp.where(here, row, 0.0), axis=1, keepdims=True)


def project(
    tokens, gain, w_query, w_key, w_value, lengths, weight,
    out, limit, owner, picked, share,
    tokens_in, gain_in, query_in, key_in, value_in, lengths_in, weight_in, sems,
):
    pairs = (
        (tokens, tokens_in),
        (gain, gain_in),
        (w_query, query_in),
        (w_key, key_in),
        (w_value, value_in),
        (lengths, lengths_in),
        (weight, weight_in),
    )
    copies = [pltpu.make_async_copy(a, b, sems.at[i]) for i, (a, b) in enumerate(pairs)]
    for copy in copies:
        copy.start()
    z, y, even = lax.axis_index("z"), lax.axis_index("y"), lax.axis_index("tp") % 2 == 0
    u, w = spot(jnp.where(even, y, z)), spot(jnp.where(even, z, y))
    half, head = u // 4, u % 4
    start = (z * 8 + y) * 128
    mine = half * 8 + w
    row_head = iota((8, 128), 0) >> 1
    same_head = (iota((8, 128), 1) & 3) == row_head
    for b in range(16):
        own_row = jnp.logical_and(mine == b, row_head == head)
        owner[8 * b : 8 * b + 8, :] = jnp.where(own_row, 1, 0)
    picked[...] = jnp.where(iota((16, 128), 0) == mine, 1.0, 0.0)
    for copy in copies[:3]:
        copy.wait()
    x = tokens_in[...].astype(F32)
    scaled = (x * gain_in[...]).astype(BF)
    query = dot(scaled, query_in[...]).astype(BF)
    copies[3].wait()
    key = dot(scaled, key_in[...])
    copies[4].wait()
    value = dot(scaled, value_in[...])
    squares = as_row(jnp.sum(x * x, axis=1, keepdims=True))
    squares = jnp.broadcast_to(squares, (8, 128)).astype(BF)
    for i in range(8):
        rows = slice(8 * (i // 4), 8 * (i // 4) + 8)
        lanes = slice(128 * (i % 4), 128 * (i % 4) + 128)
        for h in range(4):
            out[i, 16 * h : 16 * h + 16, :] = query[:, 128 * h : 128 * h + 128]
        out[i, 64:80, :] = jnp.concatenate([key[rows, lanes], value[rows, lanes]], axis=0).astype(BF)
        out[i, 80:88, :] = squares
    for copy in copies[5:]:
        copy.wait()
    for b in range(16):
        limit[8 * b : 8 * b + 8, :] = jnp.where(same_head, lengths_in[b] - start, 0)
    lane_head = (iota((8, 128), 1) >> 1) & 3
    low = jnp.where(lane_head == 0, weight_in[0], weight_in[1])
    high = jnp.where(lane_head == 2, weight_in[2], weight_in[3])
    share[...] = jnp.where(lane_head < 2, low, high)


def relay(got, out):
    total = summed(got).astype(BF)
    for i in range(8):
        out[i] = total


def relay_query(got, out):
    total = summed(got)
    query = total[0:64].astype(BF)
    row = iota((8, 128), 0)
    for i in range(8):
        out[i, 0:64, :] = query
        key = total[64 + i : 65 + i]
        value = total[72 + i : 73 + i]
        last = jnp.where(row == 0, key, jnp.where(row == 1, value, total[80:81]))
        out[i, 64:72, :] = last.astype(BF)


def attend(got, keys, values, limit, owner, picked, out, rows_q, scores, acc):
    total = summed(got)
    inverse = lax.rsqrt(as_column(total[66:67]) / 4096 + EPS)
    first = iota((16, 128), 1) < 64
    for h in range(4):
        query = rounded(inverse * total[16 * h : 16 * h + 16])
        rows_q[pl.ds(2 * h, 16, stride=8), :] = jnp.where(first, query, 0.0)
        rows_q[pl.ds(2 * h + 1, 16, stride=8), :] = jnp.where(first, 0.0, query)
    for b in range(16):
        at = slice(8 * b, 8 * b + 8)
        scores[at, :] = dot_t(rows_q[at, :].astype(BF), keys[b])
    scale = jnp.sum(inverse * picked[...], axis=0, keepdims=True)
    key_new = rounded(scale * total[64:65])
    value_new = rounded(scale * total[65:66])
    owned = owner[...] > 0
    own = jnp.sum(rows_q[...] * key_new, axis=1, keepdims=True) * 0.125
    own = jnp.where(owned, own, FLOOR_SCORE)
    lane = iota((128, 128), 1)
    tiles, seen = [], []
    peak = own
    for t in range(4):
        visible = (lane + 128 * t) >> 2 < limit[...]
        tile = jnp.where(visible, scores[:, 128 * t : 128 * t + 128] * 0.125, FLOOR_SCORE)
        tiles.append(tile)
        seen.append(visible)
        peak = jnp.maximum(peak, tile)
    peak = jnp.max(peak, axis=1, keepdims=True)
    peak_hi = rounded(peak)
    peak_lo = rounded(peak - peak_hi)
    base = peak_hi + peak_lo
    weights = [jnp.where(v, jnp.exp(t - base), 0.0) for t, v in zip(tiles, seen)]
    own_weight = jnp.where(owned, jnp.exp(own - base), 0.0)
    totals = jnp.sum(weights[0] + weights[1] + weights[2] + weights[3], axis=1, keepdims=True)
    totals = totals + own_weight
    weights = jnp.concatenate(weights, axis=1).astype(BF)
    for b in range(16):
        at = slice(8 * b, 8 * b + 8)
        acc[at, :] = dot(weights[at, :], values[b])
    body = (acc[...] + rounded(own_weight) * value_new).T.astype(BF)
    totals_hi = rounded(totals)
    stat = jnp.where(
        lane == 0,
        peak_hi,
        jnp.where(lane == 1, peak_lo, jnp.where(lane == 2, totals_hi, totals - totals_hi)),
    )
    tail = stat.T[0:8].astype(BF)
    for i in range(8):
        out[i, 0:128, :] = body
        out[i, 128:136, :] = tail


def merged(got):
    tails = [got[i, 128:136, :].astype(F32) for i in range(8)]
    peaks = [t[0:1] + t[1:2] for t in tails]
    peak = peaks[0]
    for p in peaks[1:]:
        peak = jnp.maximum(peak, p)
    totals = jnp.zeros_like(peak)
    values = jnp.zeros((128, 128), F32)
    for i in range(8):
        scale = jnp.exp(peaks[i] - peak)
        totals = totals + scale * (tails[i][2:3] + tails[i][3:4])
        values = values + scale * got[i, 0:128, :].astype(F32)
    return peak, totals, values


def merge(got, out):
    peak, totals, values = merged(got)
    peak_hi, totals_hi = rounded(peak), rounded(totals)
    row = iota((8, 128), 0)
    tail = jnp.where(
        row == 0,
        peak_hi,
        jnp.where(row == 1, peak - peak_hi, jnp.where(row == 2, totals_hi, totals - totals_hi)),
    ).astype(BF)
    body = values.astype(BF)
    for i in range(8):
        out[i, 0:128, :] = body
        out[i, 128:136, :] = tail


def mix(got, share, head_gain, w_out, out, rows):
    _, totals, values = merged(got)
    ratio = values / totals
    mixture = ratio - share[0:1] * pltpu.roll(ratio, 127, 1)
    scale = lax.rsqrt(jnp.mean(mixture * mixture, axis=0, keepdims=True) + EPS)
    rows[...] = (mixture * scale).T * head_gain[...]
    attended = jnp.concatenate(
        [rows[pl.ds(2 * h, 16, stride=8), :] for h in range(4)], axis=1
    ).astype(BF)
    term = folded(dot_t(attended, w_out[...]))
    for i in range(8):
        out[i] = term


def widen(got, tokens, gain, w_gate, w_up, out, residual_out, rows):
    residual = (tokens[...].astype(F32) + unfolded(summed(got))).astype(BF)
    residual_out[...] = residual
    x = residual.astype(F32)
    scaled = (x * gain[...]).astype(BF)
    squares = jnp.broadcast_to(jnp.sum(x * x, axis=1, keepdims=True), (16, 128))
    for first, product in ((0, dot(scaled, w_gate[...])), (24, dot(scaled, w_up[...]))):
        for t in range(12):
            tile = product[:, 128 * t : 128 * t + 128] if t < 11 else squares
            rows[pl.ds(first + 2 * t, 8, stride=48), :] = tile[0:8]
            rows[pl.ds(first + 2 * t + 1, 8, stride=48), :] = tile[8:16]
    out[...] = rows[...].astype(BF)


def activate(got, out):
    total = summed(got)
    squares = jnp.where((iota((24, 128), 0) & 1) == 0, total[22:23], total[23:24])
    inverse = lax.rsqrt(squares / 4096 + EPS)
    gate = inverse * total[0:24]
    up = inverse * total[24:48]
    hidden = (gate / (1.0 + jnp.exp(-gate)) * up).astype(BF)
    for i in range(8):
        out[i] = hidden


def narrow(got, w_down, out, rows):
    rows[...] = got[...].astype(F32)
    halves = [
        jnp.concatenate([rows[pl.ds(2 * t + i, 8, stride=24), :] for t in range(11)], axis=1)
        for i in range(2)
    ]
    hidden = jnp.concatenate(halves, axis=0).astype(BF)
    term = folded(dot_t(hidden, w_down[...]))
    for i in range(8):
        out[i] = term


def finish(got, residual, out):
    out[...] = (residual[...].astype(F32) + unfolded(summed(got))).astype(BF)


def local(
    tokens,
    attn_gain,
    w_query,
    w_key,
    w_value,
    key_cache,
    value_cache,
    lengths,
    mix_weight,
    head_gain,
    w_out,
    mixer_gain,
    w_gate,
    w_up,
    w_down,
):
    tile = pltpu.VMEM((128, 128), F32)
    sent, limit, owner, picked, share = run(
        project,
        (
            shape(8, 88, 128),
            shape(128, 128, kind=jnp.int32),
            shape(128, 128, kind=jnp.int32),
            shape(16, 128, kind=F32),
            shape(8, 128, kind=F32),
        ),
        (
            tokens,
            attn_gain[None],
            w_query,
            w_key,
            w_value,
            lengths,
            mix_weight,
        ),
        specs=[HBM] * 7,
        scratch=[
            pltpu.VMEM((16, 64), BF),
            pltpu.VMEM((1, 64), F32),
            pltpu.VMEM((64, 512), BF),
            pltpu.VMEM((64, 512), BF),
            pltpu.VMEM((64, 512), BF),
            pltpu.SMEM((16,), jnp.int32),
            pltpu.SMEM((4,), F32),
            pltpu.SemaphoreType.DMA((7,)),
        ],
    )
    sent = run(relay_query, shape(8, 72, 128), (exchange(sent, ALL, U),))
    sent = run(
        attend,
        shape(8, 136, 128),
        (
            exchange(sent, ALL, W),
            key_cache.reshape(16, 512, 128),
            value_cache.reshape(16, 512, 128),
            limit,
            owner,
            picked,
        ),
        scratch=[tile, pltpu.VMEM((128, 512), F32), tile],
    )
    sent = run(merge, shape(8, 136, 128), (exchange(sent, ALL, W),))
    sent = run(
        mix,
        shape(8, 8, 128),
        (exchange(sent, ALL, U), share, head_gain[None], w_out.T),
        scratch=[tile],
    )
    sent, residual = run(
        widen,
        (shape(384, 128), shape(16, 64)),
        (exchange(sent, "tp"), tokens, mixer_gain[None], w_gate, w_up),
        scratch=[pltpu.VMEM((384, 128), F32)],
    )
    sent = run(relay, shape(8, 48, 128), (exchange(sent.reshape(8, 48, 128), ALL, U),))
    sent = run(activate, shape(8, 24, 128), (exchange(sent, ALL, W),))
    sent = run(
        narrow,
        shape(8, 8, 128),
        (exchange(sent, ALL, U).reshape(192, 128), w_down.T),
        scratch=[pltpu.VMEM((192, 128), F32)],
    )
    return run(finish, jax.ShapeDtypeStruct((16, 64), BF), (exchange(sent, "tp"), residual))


def solution(mesh):
    finer = Mesh(mesh.devices.reshape(8, 8, mesh.shape["tp"]), ("z", "y", "tp"))
    return jax.shard_map(
        local,
        mesh=finer,
        in_specs=(
            P(None, KV),
            P(KV),
            P(KV, "tp"),
            P(KV, "tp"),
            P(KV, "tp"),
            P(None, KV, "tp", None),
            P(None, KV, "tp", None),
            P(),
            P("tp"),
            P(),
            P("tp", KV),
            P(KV),
            P(KV, "tp"),
            P(KV, "tp"),
            P("tp", KV),
        ),
        out_specs=P(None, KV),
        check_vma=False,
    )
```
